32 devices in a mesh: sp: 8 (over z, y), dp: 4 (over x, core).
Axes of the slice: x: 2, y: 2, z: 4, core: 2. Of those that a mesh axis runs over, the one named last changes fastest.
Arguments:
- query: bfloat16 [4, 1536, 3072], P('dp', 'sp'), may hold values from -18 to 18
- latent: bfloat16 [4, 1536, 1024], P('dp', 'sp'), may hold values from -6 to 6
- rope_key: bfloat16 [4, 1536, 32], P('dp', 'sp'), may hold values from -5 to 5
- latent_norm_gain: float32 [1024], replicated, may hold values from 0.1 to 1.9
- key_up_matrix: bfloat16 [2048, 1024], P('dp'), may hold values from -0.1875 to 0.1875
- value_up_matrix: bfloat16 [2048, 1024], P('dp'), may hold values from -0.1875 to 0.1875
- out_grad: bfloat16 [4, 1536, 2048], P('dp', 'sp'), may hold values from -6 to 6
Outputs:
- query_grad: bfloat16 [4, 1536, 3072], P('dp', 'sp')
- latent_grad: float32 [4, 1536, 1024], P('dp', 'sp')
- rope_key_grad: float32 [4, 1536, 32], P('dp', 'sp')
- key_weight_grad: float32 [2048, 1024], P('dp')
- value_weight_grad: float32 [2048, 1024], P('dp')
- gain_grad: float32 [1024], replicated
The draws below stay inside these ranges and needn't reach their ends.
All inputs are finite; a program needn't handle non-finite values.
Results may differ from the reference program's by a relative error of at most 0.011.
Values may be sent and summed in bfloat16 or wider, within the bound.
A program may use at most 256 MiB of HBM per device.

```python
import jax
import jax.numpy as jnp
from jax import lax

ATTENTION_HEADS = 32
PLAIN_HEAD_WIDTH = 64
ROPE = 32
VALUE_HEAD_WIDTH = 64
LATENT_WIDTH = 1024
SPAN = 64
SEQUENCE_LENGTH = 1536
BATCH_SEQUENCES = 4


def draw_rope_key(key, part):
    own = jax.random.fold_in(key, 11)
    values = jnp.clip(jax.random.normal(own, (BATCH_SEQUENCES, SEQUENCE_LENGTH, ROPE), jnp.float32), -5.0, 5.0)
    return values.astype(jnp.bfloat16)


def draw_query(key, part):
    own = jax.random.fold_in(key, 23)
    shape = (BATCH_SEQUENCES, SEQUENCE_LENGTH, ATTENTION_HEADS, PLAIN_HEAD_WIDTH + ROPE)
    values = jnp.clip(jax.random.normal(own, shape, jnp.float32), -5.0, 5.0)
    return values.reshape(BATCH_SEQUENCES, SEQUENCE_LENGTH, ATTENTION_HEADS * (PLAIN_HEAD_WIDTH + ROPE)).astype(jnp.bfloat16)


def block_scale(own_key, shape, split, least, high):
    loudness, own = 1.0, jax.random.fold_in(own_key, 6)
    for axis_at, blocks in split:
        steps = jnp.exp(jax.random.uniform(jax.random.fold_in(own, axis_at), (blocks,), jnp.float32, least / len(split), high / len(split)))
        loudness = loudness * jnp.repeat(steps, shape[axis_at] // blocks).reshape([-1 if axis == axis_at else 1 for axis in range(len(shape))])
    return loudness


def centred(rng, dims, scale, reach, split=(), held_as=jnp.bfloat16):
    result = scale * jax.random.normal(rng, dims, jnp.float32)
    if split:
        result = result * block_scale(rng, dims, split, -0.22, 0.18)
    return jnp.clip(result, -reach, reach).astype(held_as)


def setup_inputs(seed: int = 0) -> dict:
    streams_of = jax.random.split(jax.random.key(seed), 8)
    query = draw_query(jax.random.fold_in(streams_of[7], 71), 0)
    latent = centred(streams_of[1], (BATCH_SEQUENCES, SEQUENCE_LENGTH, LATENT_WIDTH), 1.0, 6.0, ((0, 4), (1, 8)))
    rope_key = draw_rope_key(jax.random.fold_in(streams_of[7], 71), 0)
    latent_norm_gain = jnp.clip(1.0 + 0.18 * jax.random.normal(streams_of[3], (LATENT_WIDTH,), jnp.float32), 0.1, 1.9)
    key_up_matrix = centred(streams_of[4], (ATTENTION_HEADS * PLAIN_HEAD_WIDTH, LATENT_WIDTH), LATENT_WIDTH ** -0.5, 0.1875, ((0, 4),))
    value_up_matrix = centred(streams_of[5], (ATTENTION_HEADS * VALUE_HEAD_WIDTH, LATENT_WIDTH), LATENT_WIDTH ** -0.5, 0.1875, ((0, 4),))
    out_grad = centred(streams_of[6], (BATCH_SEQUENCES, SEQUENCE_LENGTH, ATTENTION_HEADS * VALUE_HEAD_WIDTH), 1.0, 6.0, ((0, 4), (1, 8)))
    return {"query": query, "latent": latent, "rope_key": rope_key, "latent_norm_gain": latent_norm_gain, "key_up_matrix": key_up_matrix, "value_up_matrix": value_up_matrix, "out_grad": out_grad}


eps = 1e-06
rope_base = 10000.0

def rotate(values, cosine, sine):
    half = values.shape[-1] // 2
    first = values[..., :half]
    second = values[..., half:]
    return jnp.concatenate([first * cosine - second * sine, second * cosine + first * sine], axis=-1)

def angles(length, width):
    inverse = 1.0 / rope_base ** (jnp.arange(0, width, 2, dtype=jnp.float32) / width)
    turned = jnp.arange(length, dtype=jnp.float32)[:, None] * inverse[None, :]
    return (jnp.cos(turned), jnp.sin(turned))

def reference(query, latent, rope_key, latent_norm_gain, key_up_matrix, value_up_matrix, out_grad):
    f32 = jnp.float32
    bf16 = jnp.bfloat16
    length = SEQUENCE_LENGTH
    width = PLAIN_HEAD_WIDTH + ROPE
    scale = width ** (-0.5)
    block = 512 if length % 512 == 0 else length
    cosine, sine = angles(length, ROPE)
    neg = jnp.finfo(f32).min

    def one_sequence(inputs):
        seq_query, seq_latent, seq_rope, seq_grad = inputs
        lat = seq_latent.astype(f32)
        inv_rms = lax.rsqrt(lax.optimization_barrier(jnp.mean(lat * lat, axis=-1, keepdims=True)) + eps)
        normed = lat * inv_rms
        nlat = (normed * latent_norm_gain).astype(bf16)
        key_nope = jnp.dot(nlat, key_up_matrix.T, preferred_element_type=f32).astype(bf16).reshape(length, ATTENTION_HEADS, PLAIN_HEAD_WIDTH)
        values = jnp.dot(nlat, value_up_matrix.T, preferred_element_type=f32).astype(bf16).reshape(length, ATTENTION_HEADS, VALUE_HEAD_WIDTH)
        heads_query = seq_query.reshape(length, ATTENTION_HEADS, width)
        q_nope = heads_query[:, :, :PLAIN_HEAD_WIDTH]
        q_rope = rotate(heads_query[:, :, PLAIN_HEAD_WIDTH:].astype(f32), cosine[:, None, :], sine[:, None, :]).astype(bf16)
        k_rope = rotate(seq_rope.astype(f32), cosine, sine).astype(bf16)
        d_out = seq_grad.reshape(length, ATTENTION_HEADS, VALUE_HEAD_WIDTH)
        dk_nope = jnp.zeros((length, ATTENTION_HEADS, PLAIN_HEAD_WIDTH), f32)
        dk_rope = jnp.zeros((length, ROPE), f32)
        d_vals = jnp.zeros((length, ATTENTION_HEADS, VALUE_HEAD_WIDTH), f32)
        dq_parts = []
        for begin in range(0, length, block):
            end = begin + block
            qn = q_nope[begin:end].astype(f32)
            qr = q_rope[begin:end].astype(f32)
            go = d_out[begin:end].astype(f32)
            kn = key_nope[:end].astype(f32)
            kr = k_rope[:end].astype(f32)
            vv = values[:end].astype(f32)
            scores = (jnp.einsum('qhd,khd->hqk', qn, kn) + jnp.einsum('qhd,kd->hqk', qr, kr)) * scale
            q_seg = jnp.arange(begin, end) // SPAN
            k_seg = jnp.arange(end) // SPAN
            allowed = k_seg[None, :] <= q_seg[:, None]
            scores = jnp.where(allowed[None], scores, neg)
            probs = jax.nn.softmax(scores, axis=-1)
            d_probs = jnp.einsum('qhd,khd->hqk', go, vv)
            d_scores = probs * (d_probs - lax.optimization_barrier(jnp.sum(probs * d_probs, axis=-1, keepdims=True)))
            ds_b = d_scores.astype(bf16).astype(f32)
            p_b = probs.astype(bf16).astype(f32)
            dq_n = jnp.einsum('hqk,khd->qhd', ds_b, kn) * scale
            dq_r = jnp.einsum('hqk,kd->qhd', ds_b, kr) * scale
            dq_r = rotate(dq_r, cosine[begin:end, None, :], -sine[begin:end, None, :])
            dq_parts.append(jnp.concatenate([dq_n, dq_r], axis=-1).astype(bf16))
            dk_nope = dk_nope.at[:end].add(jnp.einsum('hqk,qhd->khd', ds_b, qn) * scale)
            dk_rope = dk_rope.at[:end].add(jnp.einsum('hqk,qhd->kd', ds_b, qr) * scale)
            d_vals = d_vals.at[:end].add(jnp.einsum('hqk,qhd->khd', p_b, go))
        query_grad = jnp.concatenate(dq_parts, axis=0).reshape(length, ATTENTION_HEADS * width)
        rope_grad = rotate(dk_rope, cosine, -sine)
        dk_b = dk_nope.astype(bf16).reshape(length, ATTENTION_HEADS * PLAIN_HEAD_WIDTH)
        dv_b = d_vals.astype(bf16).reshape(length, ATTENTION_HEADS * VALUE_HEAD_WIDTH)
        d_nlat = jnp.dot(dk_b, key_up_matrix, preferred_element_type=f32) + jnp.dot(dv_b, value_up_matrix, preferred_element_type=f32)
        key_part = jnp.dot(dk_b.T, nlat, preferred_element_type=f32)
        value_part = jnp.dot(dv_b.T, nlat, preferred_element_type=f32)
        gain_part = lax.optimization_barrier(jnp.sum(d_nlat * normed, axis=0))
        scaled = d_nlat * latent_norm_gain
        latent_grad = inv_rms * (scaled - normed * lax.optimization_barrier(jnp.mean(scaled * normed, axis=-1, keepdims=True)))
        return (query_grad, latent_grad, rope_grad, key_part, value_part, gain_part)
    results = lax.map(one_sequence, (query, latent, rope_key, out_grad))
    query_grad, latent_grad, rope_grad, key_parts, value_parts, gain_parts = results
    return (query_grad, latent_grad, rope_grad, lax.optimization_barrier(jnp.sum(key_parts, axis=0)), lax.optimization_barrier(jnp.sum(value_parts, axis=0)), lax.optimization_barrier(jnp.sum(gain_parts, axis=0)))
```

```python
import functools, math
import numpy as np
import jax, jax.numpy as jnp
from jax import lax
from jax.experimental import pallas as pl
from jax.experimental.pallas import tpu as pltpu
from jax.sharding import PartitionSpec as P
ATTENTION_HEADS = 32
PLAIN = 64
ROPE = 32
VALUE = 64
SPAN = 64
WIDTH = PLAIN + ROPE
LANES = 128
NT = (((1,), (1,)), ((), ()))
NN = (((1,), (0,)), ((), ()))
f32=jnp.float32; bf16=jnp.bfloat16
CH=64
MESH = pl.DeviceIdType.MESH
eps = 1e-06

NT = (((1,), (1,)), ((), ()))
TN = (((0,), (0,)), ((), ()))

def inner(n):
    return 2 ** ((n.bit_length() - 1) // 2)

def rcopy(src, dst, send, recv, dev):
    return pltpu.make_async_remote_copy(src_ref=src, dst_ref=dst, send_sem=send, recv_sem=recv, device_id=dev, device_id_type=MESH)

class Gather:
    def __init__(self, own, at, na, nb, a, b, dev, send, recv):
        self.own, self.at, self.na, self.nb, self.a, self.b, self.dev, self.send, self.recv = own, at, na, nb, a, b, dev, send, recv
        self.me = a * nb + b
    def copy(self, src, slot, way):
        a, b = self.a, self.b
        to = [(a + 1, b), (a - 1, b), (a, b + 1), (a, b - 1)][way]
        return rcopy(src, self.at(slot), self.send.at[slot, way], self.recv.at[slot], self.dev(*to))
    def can(self, way):
        return [self.a < self.na - 1, self.a > 0, self.b < self.nb - 1, self.b > 0][way]
    def go(self, src, slot, ways):
        for w in ways:
            @pl.when(self.can(w))
            def _(): self.copy(src, slot, w).start()
    def wait(self, slot):
        self.copy(self.own, slot, 0).wait_recv()
    def begin(self):
        self.go(self.own, self.me, (0, 1, 2, 3))
    def line(self, k, got=None):
        for sign, way in ((-1, 0), (1, 1)):
            far = self.a + sign * k
            ok = far >= 0 if sign < 0 else far < self.na
            @pl.when(ok)
            def _():
                slot = far * self.nb + self.b
                self.wait(slot)
                self.go(self.at(slot), slot, (way, 2, 3))
                if got is not None: got(slot)
    def across(self, j, got=None):
        for sign, way in ((-1, 2), (1, 3)):
            far = self.b + sign * j
            ok = far >= 0 if sign < 0 else far < self.nb
            @pl.when(ok)
            def _():
                for aa in range(self.na):
                    slot = aa * self.nb + far
                    self.wait(slot)
                    self.go(self.at(slot), slot, (way,))
                    if got is not None: got(slot)
    def finish(self):
        for w in range(4):
            @pl.when(self.can(w))
            def _(): self.copy(self.own, self.me, w).wait_send()
        for k in range(1, self.na):
            for sign, way in ((-1, 0), (1, 1)):
                far = self.a + sign * k
                ok = far >= 0 if sign < 0 else far < self.na
                @pl.when(ok)
                def _():
                    slot = far * self.nb + self.b
                    for w in (way, 2, 3):
                        @pl.when(self.can(w))
                        def _(): self.copy(self.own, slot, w).wait_send()
        for j in range(1, self.nb - 1):
            for sign, way in ((-1, 2), (1, 3)):
                far = self.b + sign * j
                ok = far >= 0 if sign < 0 else far < self.nb
                @pl.when(ok)
                def _():
                    for aa in range(self.na):
                        slot = aa * self.nb + far
                        @pl.when(self.can(way))
                        def _(): self.copy(self.own, slot, way).wait_send()

def greet(n, m, s, d):
    b = pltpu.get_barrier_semaphore()
    for k in range(1, n):
        pl.semaphore_signal(b, inc=1, device_id=(lax.rem(s + k, n), d), device_id_type=MESH)
    for k in range(1, m):
        pl.semaphore_signal(b, inc=1, device_id=(s, lax.rem(d + k, m)), device_id_type=MESH)
    pl.semaphore_wait(b, n + m - 2)

def front_kernel(n, m, chunks, packed, nlat, kw, vw, arrived, nlat_all, k_all, v_all,
                 lsem, nsend, nrecv, wsend, wrecv, qsend, qrecv):
    s = lax.axis_index("sp"); d = lax.axis_index("dp")
    ny = inner(n)
    ratio = n // m
    rows = kw.shape[0] // ratio
    z, y = lax.div(s, ny), lax.rem(s, ny)
    x, c = lax.div(d, 2), lax.rem(d, 2)
    locals_ = [pltpu.make_async_copy(packed.at[s], arrived.at[s], lsem.at[0]),
               pltpu.make_async_copy(nlat, nlat_all.at[s], lsem.at[1]),
               pltpu.make_async_copy(kw, k_all.at[d], lsem.at[2]),
               pltpu.make_async_copy(vw, v_all.at[d], lsem.at[3])]
    for l in locals_: l.start()
    greet(n, m, s, d)
    g = Gather(nlat, lambda t: nlat_all.at[t], n // ny, ny, z, y, lambda a, b: (a * ny + b, d), nsend, nrecv)
    ws = []
    for j in range(ratio):
        part = pl.ds(lax.rem(s + j, ratio) * rows, rows)
        for i, (own, whole) in enumerate(((kw, k_all), (vw, v_all))):
            ws.append(Gather(own.at[part], lambda t, whole=whole, part=part: whole.at[t, part], m // 2, 2, x, c, lambda a, b: (s, a * 2 + b), wsend.at[2 * j + i], wrecv.at[2 * j + i]))
    g.begin()
    for w in ws: w.begin()
    cs = []
    for i, (lo, hi) in enumerate(chunks):
        for k in range(1, n):
            t = lax.rem(s + k, n)
            cp = rcopy(packed.at[t, :, lo:hi], arrived.at[s, :, lo:hi], qsend.at[i, k], qrecv.at[i, k], (t, d))
            cs.append(cp)
    late = len(cs)
    for cp in cs[:0]: cp.start()
    for k in range(1, n // ny): g.line(k)
    for cp in cs: cp.start()
    for w in ws:
        for k in range(1, m // 2): w.line(k)
    for j in range(1, ny): g.across(j)
    for w in ws: w.across(1)
    for cp in cs: cp.wait()
    g.finish()
    for w in ws: w.finish()
    for l in locals_: l.wait()

def front(packed, nlat, kw, vw, m, chunks, cid=11):
    n = packed.shape[0]
    ratio = n // m
    A = pl.BlockSpec(memory_space=pl.ANY)
    S = pltpu.SemaphoreType.DMA
    outs = (jax.ShapeDtypeStruct(packed.shape, bf16), jax.ShapeDtypeStruct((n, *nlat.shape), bf16),
            jax.ShapeDtypeStruct((m, *kw.shape), bf16), jax.ShapeDtypeStruct((m, *vw.shape), bf16))
    return pl.pallas_call(
        functools.partial(front_kernel, n, m, chunks), out_shape=outs, in_specs=[A] * 4, out_specs=(A,) * 4,
        scratch_shapes=[S((4,)), S((n, 4)), S((n,)), S((2 * ratio, m, 4)), S((2 * ratio, m)), S((len(chunks), n)), S((len(chunks), n))],
        compiler_params=pltpu.CompilerParams(collective_id=cid, has_side_effects=True, vmem_limit_bytes=60 * 1024 * 1024),
    )(packed, nlat, kw, vw)

def back_kernel(n, m, dq, dk, dv, dr, part, dq_in, dk_in, dv_in, dr_in, wg_all,
                pieces, summed, blocks, lsem, psend, precv, gsend, grecv, osend, orecv, rsend, rrecv):
    s = lax.axis_index("sp"); d = lax.axis_index("dp")
    ny = inner(n)
    ratio = n // m
    z, y = lax.div(s, ny), lax.rem(s, ny)
    tokens = dq.shape[1]
    greet(n, m, s, d)
    ps = []
    for k in range(1, m):
        t = lax.rem(d + k, m)
        ps.append(rcopy(part.at[t], pieces.at[k], psend.at[k], precv.at[k], (s, t)))
    for cp in ps: cp.start()
    own = pltpu.make_async_copy(part.at[d], pieces.at[0], lsem.at[0]); own.start()
    cs = []
    moves = ((dr, dr_in), (dk, dk_in), (dv, dv_in), (dq, dq_in))
    for i, (src, dst) in enumerate(moves):
        for k in range(1, n):
            t = lax.rem(s + k, n)
            cs.append(rcopy(src.at[t], dst.at[s], rsend.at[i, k], rrecv.at[i, k], (t, d)))
    ls = [pltpu.make_async_copy(src.at[s], dst.at[s], lsem.at[1 + i]) for i, (src, dst) in enumerate(moves)]
    for l in ls: l.start()
    own.wait()
    for cp in ps: cp.wait()
    total = pieces[0].astype(f32)
    for k in range(1, m): total = total + pieces[k].astype(f32)
    summed[...] = total.astype(bf16)
    g = Gather(summed, lambda t: blocks.at[t], n // ny, ny, z, y, lambda a, b: (a * ny + b, d), gsend, grecv)
    def pass_on(slot, src):
        owner, place = lax.div(slot, ratio), lax.rem(slot, ratio)
        @pl.when(owner != d)
        def _(): rcopy(src, wg_all.at[place, d], osend.at[slot], orecv.at[place, d], (s, owner)).start()
        @pl.when(owner == d)
        def _(): pltpu.make_async_copy(src, wg_all.at[place, d], osend.at[slot]).start()
    g.begin()
    pass_on(s, summed)
    for cp in cs: cp.start()
    for k in range(1, n // ny): g.line(k, lambda slot: pass_on(slot, blocks.at[slot]))
    for j in range(1, ny): g.across(j, lambda slot: pass_on(slot, blocks.at[slot]))
    for cp in cs: cp.wait()
    g.finish()
    for slot in range(n):
        owner, place = slot // ratio, slot % ratio
        @pl.when(owner != d)
        def _(): rcopy(summed, wg_all.at[place, d], osend.at[slot], orecv.at[place, d], (s, owner)).wait_send()
        @pl.when(owner == d)
        def _(): pltpu.make_async_copy(summed, wg_all.at[place, d], osend.at[slot]).wait()
    for p in range(m):
        @pl.when(p != d)
        def _():
            for place in range(ratio):
                rcopy(summed, wg_all.at[place, p], osend.at[0], orecv.at[place, p], (s, p)).wait_recv()
    for l in ls: l.wait()

def back(dq, dk, dv, dr, part, cid=12):
    n, m = dq.shape[0], part.shape[0]
    ratio = n // m
    A = pl.BlockSpec(memory_space=pl.ANY)
    S = pltpu.SemaphoreType.DMA
    outs = tuple(jax.ShapeDtypeStruct(a.shape, a.dtype) for a in (dq, dk, dv, dr)) + (jax.ShapeDtypeStruct((ratio, *part.shape), bf16),)
    shape = part.shape[1:]
    return pl.pallas_call(
        functools.partial(back_kernel, n, m), out_shape=outs, in_specs=[A] * 5, out_specs=(A,) * 5,
        scratch_shapes=[pltpu.VMEM((m, *shape), bf16), pltpu.VMEM(shape, bf16), pltpu.VMEM((n, *shape), bf16),
                        S((5,)), S((m,)), S((m,)), S((n, 4)), S((n,)), S((n,)), S((ratio, m)), S((4, n)), S((4, n))],
        compiler_params=pltpu.CompilerParams(collective_id=cid, has_side_effects=True, vmem_limit_bytes=60 * 1024 * 1024),
    )(dq, dk, dv, dr, part)

def mm(a, b, dims=NN):
    return lax.dot_general(a, b, dims, preferred_element_type=jnp.float32)

def weave(gens):
    gens = list(gens)
    while gens:
        for g in list(gens):
            try: next(g)
            except StopIteration: gens.remove(g)

def pair_backward(tile, heads, cos_t, sin_t, s_s, dp_s, p_s, ds_s):
    length = heads[0][3].shape[0]
    blocks = length // tile
    scale = WIDTH ** (-0.5)
    steep = scale * math.log2(math.e)
    half = ROPE // 2
    query_seg = lax.broadcasted_iota(jnp.int32, (8, tile), 1) // SPAN
    def at(b): return slice(b * tile, (b + 1) * tile)
    def fold(x, op):
        return op(x.reshape(x.shape[0] // 8, 8, tile), axis=0)
    peaks = {}
    items = [(h, qi) for h in range(len(heads)) for qi in range(blocks)]
    def first(n):
        h, qi = items[n]; odd, q_s, go_s, k_s, kt_s, v_s, _, _ = heads[h]
        q = q_s[at(qi), :]; go = go_s[at(qi), :]
        par = n % 2
        peak = None
        for kb in range(qi + 1):
            s = mm(k_s[at(kb), :], q, NT)
            if kb == qi:
                parts = []
                for j in range(tile // SPAN):
                    ok = jnp.broadcast_to((query_seg >= j)[None], (SPAN // 8, 8, tile)).reshape(SPAN, tile)
                    parts.append(jnp.where(ok, s[j * SPAN:(j + 1) * SPAN], -1e30))
                s = jnp.concatenate(parts, axis=0)
            s_s[par, at(kb), :] = s
            m = fold(s, jnp.max)
            peak = m if peak is None else jnp.maximum(peak, m)
            peaks[n] = peak
            yield
            dp_s[par, at(kb), :] = mm(v_s[at(kb), :], go, NT)
            yield
    def second(n):
        h, qi = items[n]; odd, q_s, go_s, k_s, kt_s, v_s, put_dq, _ = heads[h]
        par = n % 2
        top = jnp.max(peaks[n], axis=0, keepdims=True) * steep
        total = jnp.zeros((8, tile), f32); mixed = jnp.zeros((8, tile), f32)
        for c in range((qi + 1) * tile // CH):
            r = slice(c * CH, (c + 1) * CH)
            p = jnp.exp2(s_s[par, r, :] * steep - top)
            s_s[par, r, :] = p
            total = total + fold(p, jnp.sum)
            mixed = mixed + fold(p * dp_s[par, r, :], jnp.sum)
            if c % (tile // CH) == tile // CH - 1: yield
        inverse = 1.0 / jnp.sum(total, axis=0, keepdims=True)
        delta = jnp.sum(mixed, axis=0, keepdims=True) * inverse
        for c in range((qi + 1) * tile // CH):
            r = slice(c * CH, (c + 1) * CH)
            probs = s_s[par, r, :] * inverse
            p_s[h, r, at(qi)] = probs.astype(bf16)
            ds_s[h, r, at(qi)] = (probs * (dp_s[par, r, :] - delta)).astype(bf16)
            if c % (tile // CH) == tile // CH - 1: yield
        dq = mm(kt_s[:, : (qi + 1) * tile], ds_s[h, : (qi + 1) * tile, at(qi)]) * scale
        a = 0 if odd else PLAIN
        c_, s_ = cos_t[:, at(qi)], sin_t[:, at(qi)]
        x, y = dq[a : a + half], dq[a + half : a + ROPE]
        b = PLAIN if odd else 0
        put_dq(at(qi), dq[b : b + PLAIN].astype(bf16), jnp.concatenate([x * c_ + y * s_, y * c_ - x * s_], axis=0).astype(bf16))
        yield
    def last(h):
        odd, q_s, go_s, k_s, kt_s, v_s, _, put_kv = heads[h]
        for kb in range(blocks):
            dv = mm(p_s[h, at(kb), kb * tile :], go_s[kb * tile :, :])
            dk = mm(ds_s[h, at(kb), kb * tile :], q_s[kb * tile :, :])
            put_kv(at(kb), dk * scale, dv)
            yield
    weave([first(0)])
    for n, (h, qi) in enumerate(items):
        gens = [second(n)]
        if n + 1 < len(items): gens.append(first(n + 1))
        weave(gens)
        if qi == blocks - 1: weave([last(h)])

def tables(length):
    inverse = 1.0 / 10000.0 ** (np.arange(0, ROPE, 2, dtype=np.float32) / np.float32(ROPE))
    turned = np.arange(length, dtype=np.float32)[None, :] * inverse.astype(np.float32)[:, None]
    return np.cos(turned.astype(np.float64)).astype(np.float32), np.sin(turned.astype(np.float64)).astype(np.float32)

def attention_kernel(heads, tile, arrived, keyvals, rope2, move, cos_t, sin_t, dq_out, dk_out, dv_out, dr_out,
                     q_s, k_s, kt_s, v_s, s_s, dp_s, p_s, ds_s, dqt_s, tc_s, ts_s):
    length = k_s.shape[1]
    blocks = length // tile
    lane = lax.broadcasted_iota(jnp.int32, (tile, LANES), 1)
    low = lane < PLAIN
    def at(b): return slice(b * tile, (b + 1) * tile)
    for b in range(blocks):
        z = jnp.zeros((ROPE, tile), f32)
        c = cos_t[:, at(b)]; s = sin_t[:, at(b)]
        tc_s[at(b), :] = jnp.concatenate([c, c, z, c, c, z], axis=0).T
        ts_s[at(b), :] = jnp.concatenate([-s, s, z, -s, s, z], axis=0).T
    dr_out[...] = jnp.zeros_like(dr_out)
    def pair(p, _):
        for b in range(blocks):
            x = arrived[p, at(b), :2 * LANES]
            y = mm(x, move[...])
            tc = tc_s[at(b), :]; ts = ts_s[at(b), :]
            q_s[0, at(b), :] = (y[:, :128] * jnp.where(low, 1.0, tc) + y[:, 128:256] * ts).astype(bf16)
            q_s[1, at(b), :] = (y[:, 256:384] * jnp.where(low, tc, 1.0) + y[:, 384:] * ts).astype(bf16)
            kp = keyvals[p, at(b), :]; vp = keyvals[heads // 2 + p, at(b), :]
            rp = rope2[at(b), :]
            zero = jnp.zeros_like(vp)
            ke = jnp.where(low, kp, rp); ko = jnp.where(low, rp, kp)
            k_s[0, at(b), :] = ke; k_s[1, at(b), :] = ko
            kt_s[0, :, at(b)] = ke.astype(f32).T.astype(bf16)
            kt_s[1, :, at(b)] = ko.astype(f32).T.astype(bf16)
            v_s[0, at(b), :] = jnp.where(low, vp, zero); v_s[1, at(b), :] = jnp.where(low, zero, vp)
        def put_dq(h):
            def put(cols, plain, turned):
                dqt_s[p, h * WIDTH : h * WIDTH + PLAIN, cols] = plain
                dqt_s[p, h * WIDTH + PLAIN : (h + 1) * WIDTH, cols] = turned
            return put
        def put_kv(h):
            def put(rows, dk, dv):
                if h == 0:
                    dk_out[p, rows, :] = dk.astype(bf16)
                    dv_out[p, rows, :] = dv.astype(bf16)
                    dr_out[rows, :] += jnp.where(low, 0.0, dk)
                else:
                    dk_out[p, rows, :] = jnp.where(low, dk_out[p, rows, :], dk.astype(bf16))
                    dv_out[p, rows, :] = jnp.where(low, dv_out[p, rows, :], dv.astype(bf16))
                    dr_out[rows, :] += jnp.where(low, dk, 0.0)
            return put
        go = arrived.at[p, :, 2 * LANES : 3 * LANES]
        pair_backward(tile, [(h == 1, q_s.at[h], go, k_s.at[h], kt_s.at[h], v_s.at[h], put_dq(h), put_kv(h)) for h in range(2)],
                      cos_t, sin_t, s_s, dp_s, p_s, ds_s)
        return 0
    lax.fori_loop(0, heads // 2, pair, 0)
    for p in range(heads // 2):
        for b in range(blocks):
            dq_out[at(b), p * 2 * WIDTH : (p + 1) * 2 * WIDTH] = dqt_s[p, :, at(b)].astype(f32).T.astype(bf16)

def mover():
    m = np.zeros((256, 512), np.float32)
    for h in range(2):
        base = h * WIDTH
        A = h * 256; B = A + 128
        pl_at = 64 * h; r_at = 64 - 64 * h
        for i in range(PLAIN): m[base + i, A + pl_at + i] = 1
        for i in range(ROPE):
            m[base + PLAIN + i, A + r_at + i] = 1
            m[base + PLAIN + (i + ROPE // 2) % ROPE, B + r_at + i] = 1
    return m

def attend3(arrived, keyvals, rope2, heads, tile=256):
    length = rope2.shape[0]
    pairs = heads // 2
    cos_t, sin_t = tables(length)
    V = pl.BlockSpec(memory_space=pltpu.VMEM)
    outs = (jax.ShapeDtypeStruct((length, heads * WIDTH), bf16), jax.ShapeDtypeStruct((pairs, length, 128), bf16),
            jax.ShapeDtypeStruct((pairs, length, 128), bf16), jax.ShapeDtypeStruct((length, 128), f32))
    return pl.pallas_call(
        functools.partial(attention_kernel, heads, tile), out_shape=outs,
        in_specs=[V] * 6, out_specs=(V,) * 4,
        scratch_shapes=[
            pltpu.VMEM((2, length, 128), bf16), pltpu.VMEM((2, length, 128), bf16), pltpu.VMEM((2, 128, length), bf16), pltpu.VMEM((2, length, 128), bf16),
            pltpu.VMEM((2, length, tile), f32), pltpu.VMEM((2, length, tile), f32),
            pltpu.VMEM((2, length, length), bf16), pltpu.VMEM((2, length, length), bf16),
            pltpu.VMEM((pairs, 2 * WIDTH, length), bf16), pltpu.VMEM((length, 128), f32), pltpu.VMEM((length, 128), f32),
        ],
        compiler_params=pltpu.CompilerParams(vmem_limit_bytes=60 * 1024 * 1024),
        cost_estimate=pl.CostEstimate(flops=heads * length * length * 420, bytes_accessed=8 * length * 1024, transcendentals=heads * length * length // 2),
    )(arrived, keyvals, rope2, jnp.asarray(mover(), bf16), jnp.asarray(cos_t), jnp.asarray(sin_t))

def turn(values, cosine, sine):
    half = values.shape[-1] // 2
    first = values[..., :half]
    second = values[..., half:]
    return jnp.concatenate([first * cosine - second * sine, second * cosine + first * sine], axis=-1)


def local(query, latent, rope_key, gain, key_up, value_up, out_grad):
    sp = lax.axis_size("sp")
    dp = lax.axis_size("dp")
    tokens, channels = latent.shape[1:]
    length = sp * tokens
    heads = ATTENTION_HEADS // sp
    pairs = heads // 2
    ratio = sp // dp
    s = lax.axis_index("sp")
    cos_t, sin_t = tables(length)
    cosine = lax.dynamic_slice_in_dim(jnp.asarray(cos_t.T), s * tokens, tokens, 0)
    sine = lax.dynamic_slice_in_dim(jnp.asarray(sin_t.T), s * tokens, tokens, 0)

    packed = jnp.concatenate(
        [query[0].reshape(tokens, sp, heads * WIDTH), out_grad[0].reshape(tokens, sp, heads * VALUE)], axis=-1
    ).transpose(1, 0, 2)
    lat = latent[0].astype(f32)
    inv_rms = lax.rsqrt(jnp.mean(lat * lat, axis=-1, keepdims=True) + eps)
    normed = lat * inv_rms
    nlat = (normed * gain).astype(bf16)
    k_rope = turn(rope_key[0].astype(f32), cosine, sine).astype(bf16)
    gap = jnp.zeros((tokens, ROPE), bf16)
    sent = jnp.concatenate([nlat, k_rope, gap, k_rope, gap], axis=1)
    arrived, nlat_all, k_all, v_all = front(packed, sent, key_up, value_up, dp, ((0, heads * (WIDTH + VALUE)),))

    arrived = arrived.reshape(length, -1)
    nlat_all = nlat_all.reshape(length, -1)
    rope2 = nlat_all[:, channels:]
    nlat_all = nlat_all[:, :channels]
    k_all = k_all.reshape(-1, channels)
    v_all = v_all.reshape(-1, channels)
    own = heads * PLAIN
    k_own = lax.dynamic_slice_in_dim(k_all, s * own, own, 0)
    v_own = lax.dynamic_slice_in_dim(v_all, s * own, own, 0)
    keys = lax.dot_general(nlat_all, k_own, NT, preferred_element_type=f32).astype(bf16)
    vals = lax.dot_general(nlat_all, v_own, NT, preferred_element_type=f32).astype(bf16)
    kv = jnp.stack([a[:, j * LANES : (j + 1) * LANES] for a in (keys, vals) for j in range(pairs)])
    gap = jnp.zeros((length, PLAIN), bf16)
    arr = jnp.stack([jnp.concatenate([arrived[:, p * 2 * WIDTH : (p + 1) * 2 * WIDTH], gap, arrived[:, heads * WIDTH + p * LANES : heads * WIDTH + (p + 1) * LANES]], 1) for p in range(pairs)])
    dq, dk, dv, dr = attend3(arr, kv, rope2, heads)
    dkc = jnp.concatenate([dk[p] for p in range(pairs)], 1)
    dvc = jnp.concatenate([dv[p] for p in range(pairs)], 1)
    TN = (((0,), (0,)), ((), ()))
    part = jnp.concatenate([lax.dot_general(a, nlat_all, TN, preferred_element_type=f32).astype(bf16) for a in (dkc, dvc)])
    part = part.reshape(dp, -1, channels)
    drc = (dr[:, :ROPE] + dr[:, PLAIN : PLAIN + ROPE])
    dq, dk, dv, dr, wg = back(*(a.reshape(sp, tokens, -1) for a in (dq, dkc, dvc, drc)), part)
    query_grad = dq.transpose(1, 0, 2).reshape(tokens, -1)
    dk = dk.transpose(1, 0, 2).reshape(tokens, -1)
    dv = dv.transpose(1, 0, 2).reshape(tokens, -1)
    rope_grad = turn(jnp.sum(dr, axis=0), cosine, -sine)
    wg = wg.reshape(ratio, 2, own, channels).astype(f32)
    d_nlat = lax.dot_general(dk, k_all, NN, preferred_element_type=f32)
    d_nlat = d_nlat + lax.dot_general(dv, v_all, NN, preferred_element_type=f32)
    gain_grad = lax.psum(jnp.sum(d_nlat * normed, axis=0), ("sp", "dp"))
    scaled = d_nlat * gain
    latent_grad = inv_rms * (scaled - normed * jnp.mean(scaled * normed, axis=-1, keepdims=True))
    return (query_grad[None], latent_grad[None], rope_grad[None], wg[:, 0].reshape(-1, channels), wg[:, 1].reshape(-1, channels), gain_grad)


def solution(mesh):
    tok = P("dp", "sp", None)
    rows = P("dp", None)
    return jax.shard_map(local, mesh=mesh, in_specs=(tok, tok, tok, P(), rows, rows, tok), out_specs=(tok, tok, tok, rows, rows, P()), check_vma=False)
```

```python
import functools, math
import numpy as np
import jax, jax.numpy as jnp
from jax import lax
from jax.experimental import pallas as pl
from jax.experimental.pallas import tpu as pltpu
from jax.sharding import PartitionSpec as P
ATTENTION_HEADS = 32
PLAIN = 64
ROPE = 32
VALUE = 64
SPAN = 64
WIDTH = PLAIN + ROPE
LANES = 128
NT = (((1,), (1,)), ((), ()))
NN = (((1,), (0,)), ((), ()))
f32=jnp.float32; bf16=jnp.bfloat16
CH=64
MESH = pl.DeviceIdType.MESH
eps = 1e-06


def inner(n):
    return 2 ** ((n.bit_length() - 1) // 2)

def rcopy(src, dst, send, recv, dev):
    return pltpu.make_async_remote_copy(src_ref=src, dst_ref=dst, send_sem=send, recv_sem=recv, device_id=dev, device_id_type=MESH)

class Gather:
    def __init__(self, own, at, na, nb, a, b, dev, send, recv):
        self.own, self.at, self.na, self.nb, self.a, self.b, self.dev, self.send, self.recv = own, at, na, nb, a, b, dev, send, recv
        self.me = a * nb + b
    def copy(self, src, slot, way):
        a, b = self.a, self.b
        to = [(a + 1, b), (a - 1, b), (a, b + 1), (a, b - 1)][way]
        return rcopy(src, self.at(slot), self.send.at[slot, way], self.recv.at[slot], self.dev(*to))
    def can(self, way):
        return [self.a < self.na - 1, self.a > 0, self.b < self.nb - 1, self.b > 0][way]
    def go(self, src, slot, ways):
        for w in ways:
            @pl.when(self.can(w))
            def _(): self.copy(src, slot, w).start()
    def wait(self, slot):
        self.copy(self.own, slot, 0).wait_recv()
    def begin(self):
        self.go(self.own, self.me, (0, 1, 2, 3))
    def line(self, k, got=None):
        for sign, way in ((-1, 0), (1, 1)):
            far = self.a + sign * k
            ok = far >= 0 if sign < 0 else far < self.na
            @pl.when(ok)
            def _():
                slot = far * self.nb + self.b
                self.wait(slot)
                self.go(self.at(slot), slot, (way, 2, 3))
                if got is not None: got(slot)
    def across(self, j, got=None):
        for sign, way in ((-1, 2), (1, 3)):
            far = self.b + sign * j
            ok = far >= 0 if sign < 0 else far < self.nb
            @pl.when(ok)
            def _():
                for aa in range(self.na):
                    slot = aa * self.nb + far
                    self.wait(slot)
                    self.go(self.at(slot), slot, (way,))
                    if got is not None: got(slot)
    def finish(self):
        for w in range(4):
            @pl.when(self.can(w))
            def _(): self.copy(self.own, self.me, w).wait_send()
        for k in range(1, self.na):
            for sign, way in ((-1, 0), (1, 1)):
                far = self.a + sign * k
                ok = far >= 0 if sign < 0 else far < self.na
                @pl.when(ok)
                def _():
                    slot = far * self.nb + self.b
                    for w in (way, 2, 3):
                        @pl.when(self.can(w))
                        def _(): self.copy(self.own, slot, w).wait_send()
        for j in range(1, self.nb - 1):
            for sign, way in ((-1, 2), (1, 3)):
                far = self.b + sign * j
                ok = far >= 0 if sign < 0 else far < self.nb
                @pl.when(ok)
                def _():
                    for aa in range(self.na):
                        slot = aa * self.nb + far
                        @pl.when(self.can(way))
                        def _(): self.copy(self.own, slot, way).wait_send()


def mm(a, b, dims=NN):
    return lax.dot_general(a, b, dims, preferred_element_type=jnp.float32)

def weave(gens):
    gens = list(gens)
    while gens:
        for g in list(gens):
            try: next(g)
            except StopIteration: gens.remove(g)

def pair_backward(tile, heads, cos_t, sin_t, s_s, dp_s, p_s, ds_s, dk_s=None, dv_s=None):
    length = heads[0][3].shape[0]
    blocks = length // tile
    scale = WIDTH ** (-0.5)
    steep = scale * math.log2(math.e)
    depth, held = s_s.shape[0], p_s.shape[0]
    half = ROPE // 2
    query_seg = lax.broadcasted_iota(jnp.int32, (8, tile), 1) // SPAN
    def at(b): return slice(b * tile, (b + 1) * tile)
    half_rows = (blocks + 1) // 2
    def spot(kb, qi, count=1):
        if dk_s is not None:
            return kb, slice(0, tile)
        if kb < half_rows:
            row, col = kb, qi - kb
        else:
            row, col = blocks - 1 - kb, kb + 1 + qi - kb
        return row, slice(col * tile, (col + count) * tile)
    def fold(x, op):
        return op(x.reshape(x.shape[0] // 8, 8, tile), axis=0)
    peaks = {}
    items = [(h, qi) for h in range(len(heads)) for qi in range(blocks)]
    def first(n):
        h, qi = items[n]; odd, q_s, go_s, k_s, kt_s, v_s, _, _ = heads[h]
        q = q_s[at(qi), :]; go = go_s[at(qi), :]
        par = n % depth
        peak = None
        for kb in range(qi + 1):
            s = mm(k_s[at(kb), :], q, NT)
            if kb == qi:
                parts = []
                for j in range(tile // SPAN):
                    ok = jnp.broadcast_to((query_seg >= j)[None], (SPAN // 8, 8, tile)).reshape(SPAN, tile)
                    parts.append(jnp.where(ok, s[j * SPAN:(j + 1) * SPAN], -1e30))
                s = jnp.concatenate(parts, axis=0)
            s_s[par, at(kb), :] = s
            m = fold(s, jnp.max)
            peak = m if peak is None else jnp.maximum(peak, m)
            peaks[n] = peak
            yield
            dp_s[par, at(kb), :] = mm(v_s[at(kb), :], go, NT)
            yield
    def second(n):
        h, qi = items[n]; odd, q_s, go_s, k_s, kt_s, v_s, put_dq, _ = heads[h]
        par = n % depth
        top = jnp.max(peaks[n], axis=0, keepdims=True) * steep
        total = jnp.zeros((8, tile), f32); mixed = jnp.zeros((8, tile), f32)
        for c in range((qi + 1) * tile // CH):
            r = slice(c * CH, (c + 1) * CH)
            p = jnp.exp2(s_s[par, r, :] * steep - top)
            s_s[par, r, :] = p
            total = total + fold(p, jnp.sum)
            mixed = mixed + fold(p * dp_s[par, r, :], jnp.sum)
            if c % (tile // CH) == tile // CH - 1: yield
        inverse = 1.0 / jnp.sum(total, axis=0, keepdims=True)
        delta = jnp.sum(mixed, axis=0, keepdims=True) * inverse
        for c in range((qi + 1) * tile // CH):
            r = slice(c * CH, (c + 1) * CH)
            probs = s_s[par, r, :] * inverse
            kb, inside = divmod(c * CH, tile)
            row, cols = spot(kb, qi)
            p_s[h % held, row, inside : inside + CH, cols] = probs.astype(bf16)
            ds_s[h % held, row, inside : inside + CH, cols] = (probs * (dp_s[par, r, :] - delta)).astype(bf16)
            if c % (tile // CH) == tile // CH - 1: yield
        dq = None
        for kb in range(qi + 1):
            row, cols = spot(kb, qi)
            term = mm(kt_s[:, at(kb)], ds_s[h % held, row, :, cols])
            dq = term if dq is None else dq + term
        dq = dq * scale
        a = 0 if odd else PLAIN
        c_, s_ = cos_t[:, at(qi)], sin_t[:, at(qi)]
        x, y = dq[a : a + half], dq[a + half : a + ROPE]
        b = PLAIN if odd else 0
        if dk_s is not None:
            for kb in range(qi + 1):
                row, cols = spot(kb, qi)
                for acc, left, right in ((dv_s, p_s, go_s), (dk_s, ds_s, q_s)):
                    term = mm(left[h % held, row, :, cols], right[at(qi), :])
                    if kb == qi:
                        acc[at(kb), :] = term
                    else:
                        acc[at(kb), :] += term
        put_dq(at(qi), dq[b : b + PLAIN].astype(bf16), jnp.concatenate([x * c_ + y * s_, y * c_ - x * s_], axis=0).astype(bf16))
        yield
    def last(h):
        odd, q_s, go_s, k_s, kt_s, v_s, _, put_kv = heads[h]
        for kb in range(blocks):
            if dk_s is not None:
                put_kv(at(kb), dk_s[at(kb), :] * scale, dv_s[at(kb), :])
                continue
            row, cols = spot(kb, kb, blocks - kb)
            dv = mm(p_s[h % held, row, :, cols], go_s[kb * tile :, :])
            dk = mm(ds_s[h % held, row, :, cols], q_s[kb * tile :, :])
            put_kv(at(kb), dk * scale, dv)
            yield
    weave([first(0)])
    for n, (h, qi) in enumerate(items):
        gens = [second(n)]
        if n + 1 < len(items): gens.append(first(n + 1))
        weave(gens)
        if qi == blocks - 1: weave([last(h)])

def tables(length):
    inverse = 1.0 / 10000.0 ** (np.arange(0, ROPE, 2, dtype=np.float32) / np.float32(ROPE))
    turned = np.arange(length, dtype=np.float32)[None, :] * inverse.astype(np.float32)[:, None]
    return np.cos(turned.astype(np.float64)).astype(np.float32), np.sin(turned.astype(np.float64)).astype(np.float32)

PARTS = 2


def head_mover(pairs):
    m = np.zeros((min(pairs, 2), 2 * LANES, 4 * LANES), np.float32)
    for p in range(m.shape[0]):
        for h in range(2):
            base = p * 64 + h * WIDTH
            plain, turned = PLAIN * h, PLAIN - PLAIN * h
            for i in range(PLAIN):
                m[p, base + i, 2 * LANES * h + plain + i] = 1
            for i in range(ROPE):
                m[p, base + PLAIN + i, 2 * LANES * h + turned + i] = 1
                m[p, base + PLAIN + (i + ROPE // 2) % ROPE, 2 * LANES * h + LANES + turned + i] = 1
    return m


def rope_mover():
    m = np.zeros((ROPE, 2 * LANES), np.float32)
    for i in range(ROPE):
        for at in (0, PLAIN):
            m[i, at + i] = 1
            m[(i + ROPE // 2) % ROPE, LANES + at + i] = 1
    return m


class Plan:
    def __init__(self, n, m, tokens, channels):
        self.n, self.m, self.tokens, self.channels = n, m, tokens, channels
        self.length = n * tokens
        self.heads = ATTENTION_HEADS // n
        self.pairs = self.heads // 2
        self.ratio = n // m
        self.qw = self.heads * WIDTH
        self.own = self.heads * PLAIN
        self.tile = 256
        self.blocks = self.length // self.tile
        self.depth = 2 if self.length <= 2048 else 1
        self.hold = self.length <= 2048
        self.aligned = self.qw % LANES == 0
        qt = -(-self.qw // LANES)
        if self.pairs == 2 and self.qw == 3 * LANES:
            self.chunks = ((0, 3 * LANES), (3 * LANES, 5 * LANES))
            self.q_tiles = ((0, 1), (1, 3))
            self.go_tile = (2, 4)
            self.dq_cols = ((0, LANES), (LANES, 3 * LANES))
        else:
            self.chunks = ((0, (qt + self.pairs) * LANES),)
            self.q_tiles = tuple((p * 2 * WIDTH // LANES, p * 2 * WIDTH // LANES + 1) for p in range(self.pairs))
            self.go_tile = tuple(qt + p for p in range(self.pairs))
            self.dq_cols = ((0, 0),) * (self.pairs - 1) + ((0, self.qw),)
        self.wide = self.chunks[-1][1]
        self.direct = self.pairs == 2 and self.qw == 3 * LANES
        if self.direct:
            self.moves = (((0, 0, 2 * LANES, 0), (1, 0, LANES, 2 * LANES)), ((0, 2 * LANES, LANES, 3 * LANES), (1, LANES, LANES, 4 * LANES)))
        else:
            self.moves = (((2, 0, self.wide, 0),),)
            self.chunks = ((0, self.wide),)
        self.rows = 2 * self.own // m

    def pack(self, query, grad):
        if self.direct:
            return query, grad
        q = query.reshape(self.tokens, self.n, self.qw)
        g = grad.reshape(self.tokens, self.n, self.own)
        gap = self.wide - self.qw - self.own
        parts = [q] + ([jnp.zeros((*q.shape[:2], gap), bf16)] if gap else []) + [g]
        return jnp.concatenate(parts, axis=-1).transpose(1, 0, 2), grad


def fused_kernel(
    pn,
    query, grad, latent, rope_key, gain, kw, vw, move, rmove, cos_t, sin_t,
    dq_in, wg_out, latent_out, rope_out, gain_out,
    arrived, nlat_all, k_all, v_all, q_s, go_s, k_s, kt_s, v_s, s_s, dp_s, p_s, ds_s, dqt_s, tc_s, ts_s,
    latent_grad, rope_grad, gain_grad, dk_s, dv_s, dq_send, dk_send, dv_send, dr_s, dr_send, dr_in, dk_in, dv_in, part, pieces, summed, blocks, d_nlat, g_part, g_in, g_part2, g_in2,
    lsem, nsend, nrecv, wsend, wrecv, qsend, qrecv, rsend, rrecv, psend, precv, gsend, grecv, osend, orecv, asend, arecv, bsend, brecv,
):
    n, m, tokens, channels, tile = pn.n, pn.m, pn.tokens, pn.channels, pn.tile
    length, pairs, ratio, own = pn.length, pn.pairs, pn.ratio, pn.own
    s = lax.axis_index("sp")
    d = lax.axis_index("dp")
    ny = inner(n)
    nz = n // ny
    z, y = lax.div(s, ny), lax.rem(s, ny)
    x, c = lax.div(d, 2), lax.rem(d, 2)
    scale = WIDTH ** (-0.5)

    scopes = []

    def mark(name):
        if scopes:
            scopes.pop().__exit__(None, None, None)
        if name:
            scopes.append(jax.named_scope(name))
            scopes[-1].__enter__()

    def block(t):
        return pl.ds(pl.multiple_of(t * tokens, tokens), tokens)

    def at(b):
        return slice(b * tile, (b + 1) * tile)

    def source(move, t):
        which, lo, width, _ = move
        if which == 2:
            return query.at[t]
        ref, each = (query, pn.qw) if which == 0 else (grad, own)
        return ref.at[:, pl.ds(pl.multiple_of(t * each + lo, LANES), width)]

    def landing(move, t):
        return arrived.at[block(t), move[3] : move[3] + move[2]]

    spread = [(i, move) for i, moves in enumerate(pn.moves) for move in moves]

    def local_copies():
        made = [pltpu.make_async_copy(kw, k_all.at[d], lsem.at[0]), pltpu.make_async_copy(vw, v_all.at[d], lsem.at[1])]
        return made + [pltpu.make_async_copy(source(move, s), landing(move, s), lsem.at[3 + j]) for j, (_, move) in enumerate(spread)]

    for copy in local_copies():
        copy.start()
    mark("greet")
    bar = pltpu.get_barrier_semaphore()
    for k in range(1, n):
        pl.semaphore_signal(bar, inc=1, device_id=(lax.rem(s + k, n), d), device_id_type=MESH)
    for k in range(1, m):
        pl.semaphore_signal(bar, inc=1, device_id=(s, lax.rem(d + k, m)), device_id_type=MESH)

    lat = latent[...].astype(f32)
    inv_rms = lax.rsqrt(jnp.mean(lat * lat, axis=-1, keepdims=True) + eps)
    nlat_all[block(s), :channels] = (lat * inv_rms * gain[...]).astype(bf16)
    for b in range(pn.blocks):
        none = jnp.zeros((ROPE, tile), f32)
        co, si = cos_t[:, at(b)], sin_t[:, at(b)]
        tc_s[at(b), :] = jnp.concatenate([co, co, none, co, co, none], axis=0).T
        ts_s[at(b), :] = jnp.concatenate([-si, si, none, -si, si, none], axis=0).T
    turned = mm(rope_key[...], rmove[...], (((0,), (0,)), ((), ())))
    nlat_all[block(s), channels:] = (turned[:, :LANES] * tc_s[block(s), :] + turned[:, LANES:] * ts_s[block(s), :]).astype(bf16)
    dr_s[...] = jnp.zeros_like(dr_s)
    mark("bar_wait")
    pl.semaphore_wait(bar, n + m - 2)

    def member(a, b):
        return (a * ny + b, d)

    gs = []
    cut = tokens // PARTS
    for j in range(PARTS):
        def rows_of(t, j=j):
            return nlat_all.at[pl.ds(pl.multiple_of(t * tokens + j * cut, cut), cut)]
        gs.append(Gather(rows_of(s), rows_of, nz, ny, z, y, member, nsend.at[j], nrecv.at[j]))
    ws = []
    for j in range(ratio):
        rows = pl.ds(pl.multiple_of(lax.rem(s + j, ratio) * own, own), own)
        for i, (mine, whole) in enumerate(((kw, k_all), (vw, v_all))):
            ws.append(Gather(mine.at[rows], lambda t, whole=whole, rows=rows: whole.at[t, rows], m // 2, 2, x, c,
                             lambda a, b: (s, a * 2 + b), wsend.at[2 * j + i], wrecv.at[2 * j + i]))

    def others(act):
        lax.fori_loop(1, n, lambda k, _: (act(k, lax.rem(s + k, n)), 0)[1], 0)

    def moved(chunk, k, t):
        return [rcopy(source(move, t), landing(move, s), qsend.at[j, k], qrecv.at[j, k], (t, d)) for j, (i, move) in enumerate(spread) if i == chunk]

    def start_moved(chunk, when=None):
        def act(k, t):
            def go():
                for copy in moved(chunk, k, t):
                    copy.start()
            if when is None:
                go()
            else:
                pl.when(when(lax.div(t, ny)))(go)
        others(act)

    mark("gather")
    for g in gs:
        g.begin()
    for w in ws:
        w.begin()
    for i in range(nz):
        if i:
            for g in gs:
                g.line(i)

        @pl.when(z == i)
        def _():
            start_moved(0, lambda tz: tz > z)

        @pl.when(nz - 1 - z == i)
        def _():
            start_moved(0, lambda tz: tz < z)

    start_moved(0, lambda tz: tz == z)
    for chunk in range(1, len(pn.chunks)):
        start_moved(chunk)
    mark("w_line")
    for w in ws[:2]:
        for k in range(1, m // 2):
            w.line(k)
    mark("across")
    for j in range(1, ny):
        for g in gs:
            g.across(j)
    for w in ws[:2]:
        w.across(1)
    for copy in local_copies():
        copy.wait()
    for w in ws[2:]:
        for k in range(1, m // 2):
            w.line(k)

    mark("project")
    holder = lax.div(s, ratio)
    mine = pl.ds(pl.multiple_of(lax.rem(s, ratio) * own, own), own)

    def project(b, _):
        rows = pl.ds(pl.multiple_of(b * tile, tile), tile)
        a = nlat_all[rows, :channels]
        keys = mm(a, k_all[holder, mine, :], NT).astype(bf16)
        vals = mm(a, v_all[holder, mine, :], NT).astype(bf16)
        for p in range(pairs):
            dk_send[p, rows, :] = keys[:, p * LANES : (p + 1) * LANES]
            dv_send[p, rows, :] = vals[:, p * LANES : (p + 1) * LANES]
        return 0

    lax.fori_loop(0, pn.blocks, project, 0)

    lane = lax.broadcasted_iota(jnp.int32, (tile, LANES), 1)
    low = lane < PLAIN

    def returned(p, i, k, t):
        lo, hi = pn.dq_cols[p]
        cols = pl.ds(pl.multiple_of(s * own + p * LANES, LANES), LANES)
        if i == 0:
            src, dst = dk_send.at[p, block(t)], dk_in.at[:, cols]
        elif i == 1:
            src, dst = dv_send.at[p, block(t)], dv_in.at[:, cols]
        else:
            src = dq_send.at[block(t), lo:hi]
            dst = dq_in.at[:, pl.ds(pl.multiple_of(s * pn.qw + lo, LANES), hi - lo)] if pn.aligned else dq_in.at[s]
        return rcopy(src, dst, rsend.at[3 * p + i, k], rrecv.at[3 * p + i, k], (t, d))

    def has_dq(p):
        return pn.dq_cols[p][1] > pn.dq_cols[p][0]

    def own_copies(p):
        cols = pl.ds(pl.multiple_of(s * own + p * LANES, LANES), LANES)
        dk_in[:, cols] = dk_send[p, block(s), :]
        dv_in[:, cols] = dv_send[p, block(s), :]

    def dq_own():
        if pn.aligned:
            return pltpu.make_async_copy(dq_send.at[block(s)], dq_in.at[:, pl.ds(pl.multiple_of(s * pn.qw, LANES), pn.qw)], lsem.at[2])
        return pltpu.make_async_copy(dq_send.at[block(s)], dq_in.at[s], lsem.at[2])

    def pieces_of(p):
        return [t for t in range(m) if t * pn.rows // LANES % pairs == p]

    def part_copy(t, j):
        return rcopy(part.at[t], pieces.at[j], psend.at[t], precv.at[j], (s, t))

    def weight_parts(p):
        for i, src in ((p, dk_send), (pairs + p, dv_send)):
            out = mm(src[p], nlat_all[:, :channels], (((0,), (0,)), ((), ()))).astype(bf16)
            for r in range(0, LANES, pn.rows):
                part[(i * LANES + r) // pn.rows] = out[r : r + pn.rows]
        for t in pieces_of(p):
            @pl.when(t != d)
            def _():
                part_copy(t, d).start()

    def pair(p, _):
        for q in range(pairs):
            @pl.when(p == q)
            def _():
                if q < len(pn.chunks):
                    with jax.named_scope(f"chunk_wait{q}"):
                        others(lambda k, t: [copy.wait_recv() for copy in moved(q, k, t)])
                t0, t1 = pn.q_tiles[q]

                def prepare(b, _):
                    rows = pl.ds(pl.multiple_of(b * tile, tile), tile)
                    xs = jnp.concatenate([arrived[rows, t0 * LANES : (t0 + 1) * LANES], arrived[rows, t1 * LANES : (t1 + 1) * LANES]], axis=1)
                    out = mm(xs, move[q % 2])
                    tc, ts = tc_s[rows, :], ts_s[rows, :]
                    q_s[0, rows, :] = (out[:, :LANES] * jnp.where(low, 1.0, tc) + out[:, LANES : 2 * LANES] * ts).astype(bf16)
                    q_s[1, rows, :] = (out[:, 2 * LANES : 3 * LANES] * jnp.where(low, tc, 1.0) + out[:, 3 * LANES :] * ts).astype(bf16)
                    go_s[rows, :] = arrived[rows, pn.go_tile[q] * LANES : (pn.go_tile[q] + 1) * LANES]
                    return 0

                lax.fori_loop(0, pn.blocks, prepare, 0)

        for b in range(pn.blocks):
            kp, vp, rp = dk_send[p, at(b), :], dv_send[p, at(b), :], nlat_all[at(b), channels:]
            none = jnp.zeros_like(vp)
            even, odd = jnp.where(low, kp, rp), jnp.where(low, rp, kp)
            k_s[0, at(b), :] = even
            k_s[1, at(b), :] = odd
            kt_s[0, :, at(b)] = even.astype(f32).T.astype(bf16)
            kt_s[1, :, at(b)] = odd.astype(f32).T.astype(bf16)
            v_s[0, at(b), :] = jnp.where(low, vp, none)
            v_s[1, at(b), :] = jnp.where(low, none, vp)

        def put_dq(h):
            def put(cols, plain, back):
                dqt_s[p, h * WIDTH : h * WIDTH + PLAIN, cols] = plain
                dqt_s[p, h * WIDTH + PLAIN : (h + 1) * WIDTH, cols] = back
            return put

        def put_kv(h):
            def put(rows, dk, dv):
                if h == 0:
                    dk_send[p, rows, :] = dk.astype(bf16)
                    dv_send[p, rows, :] = dv.astype(bf16)
                    dr_s[rows, :] += jnp.where(low, 0.0, dk)
                else:
                    dk_send[p, rows, :] = jnp.where(low, dk_send[p, rows, :], dk.astype(bf16))
                    dv_send[p, rows, :] = jnp.where(low, dv_send[p, rows, :], dv.astype(bf16))
                    dr_s[rows, :] += jnp.where(low, dk, 0.0)
            return put

        with jax.named_scope("core"):
          pair_backward(tile, [(h == 1, q_s.at[h], go_s, k_s.at[h], kt_s.at[h], v_s.at[h], put_dq(h), put_kv(h)) for h in range(2)],
                      cos_t, sin_t, s_s, dp_s, p_s, ds_s, *(() if pn.hold else (dk_s, dv_s)))

        for q in range(pairs):
            @pl.when(p == q)
            def _():
                lo, hi = pn.dq_cols[q]
                for b in range(pn.blocks):
                    if hi > lo:
                        rows = [dqt_s[i // (2 * WIDTH), i % (2 * WIDTH) : i % (2 * WIDTH) + 64, at(b)] for i in range(lo, hi, 64)]
                        dq_send[at(b), lo:hi] = jnp.concatenate(rows, axis=0).astype(f32).T.astype(bf16)
                if q < pairs - 1:
                    for i in range(3 if has_dq(q) else 2):
                        others(lambda k, t: returned(q, i, k, t).start())
                own_copies(q)
                weight_parts(q)
        return 0

    mark("pairs")
    lax.fori_loop(0, pairs, pair, 0)

    mark("dr")
    quarter = tokens // 4
    both = dr_s[:, :ROPE] + dr_s[:, PLAIN : PLAIN + ROPE]
    for t in range(n):
        dr_send[t] = jnp.concatenate([both[t * tokens + j * quarter : t * tokens + (j + 1) * quarter] for j in range(4)], axis=1)
    dr_in[s] = dr_send[s]

    def dr_copy(k, t):
        return rcopy(dr_send.at[t], dr_in.at[s], asend.at[1, k], arecv.at[1, k], (t, d))


    mark("part_wait")
    pieces[d] = part[d]
    for j in range(m):
        @pl.when(j != d)
        def _():
            part_copy(0, j).wait_recv()
    total = pieces[0].astype(f32)
    for j in range(1, m):
        total = total + pieces[j].astype(f32)
    summed[...] = total.astype(bf16)

    wg = Gather(summed, lambda t: blocks.at[t], nz, ny, z, y, member, gsend, grecv)

    def place_of(slot, j):
        rows = pl.ds(pl.multiple_of(lax.rem(slot, ratio) * own + lax.rem(j, m // 2) * pn.rows, pn.rows), pn.rows)
        return wg_out.at[lax.div(j, m // 2), rows]

    def pass_on(slot, src):
        owner, place = lax.div(slot, ratio), lax.rem(slot, ratio)

        @pl.when(owner != d)
        def _():
            rcopy(src, place_of(slot, d), osend.at[slot], orecv.at[place, d], (s, owner)).start()

        @pl.when(owner == d)
        def _():
            pltpu.make_async_copy(src, place_of(slot, d), osend.at[slot]).start()

    mark("wg_line")
    wg.begin()
    pass_on(s, summed)
    dq_own().start()
    final = pairs - 1
    others(lambda k, t: returned(final, 0, k, t).start())
    for i in range(1, nz):
        wg.line(i, lambda slot: pass_on(slot, blocks.at[slot]))
        if i == 1:
            others(lambda k, t: returned(final, 1, k, t).start())
        if i == min(2, nz - 1):
            others(lambda k, t: dr_copy(k, t).start())
            others(lambda k, t: returned(final, 2, k, t).start())
    mark("wg_across")
    for j in range(1, ny):
        wg.across(j, lambda slot: pass_on(slot, blocks.at[slot]))
    mark("kv_wait")
    for p in range(pairs):
        for i in range(2):
            others(lambda k, t: returned(p, i, k, t).wait_recv())
    mark("w_rest")
    for w in ws[2:]:
        w.across(1)
    mark("d_nlat")
    for t in range(m):
        cols = slice(t * ratio * own, (t + 1) * ratio * own)
        term = mm(dk_in[:, cols], k_all[t]) + mm(dv_in[:, cols], v_all[t])
        if t == 0:
            d_nlat[...] = term
        else:
            d_nlat[...] += term
    lat = latent[...].astype(f32)
    inv_rms = lax.rsqrt(jnp.mean(lat * lat, axis=-1, keepdims=True) + eps)
    normed = lat * inv_rms
    dn = d_nlat[...]
    sums = jnp.sum(dn * normed, axis=0, keepdims=True)
    g_part[...] = jnp.concatenate([sums[:, i * LANES : (i + 1) * LANES] for i in range(channels // LANES)], axis=0)

    def first_round(k, t):
        return rcopy(g_part, g_in.at[k], asend.at[0, k], arecv.at[0, k], (t, d))

    others(lambda k, t: first_round(k, t).start())
    scaled = dn * gain[...]
    latent_grad[...] = inv_rms * (scaled - normed * jnp.mean(scaled * normed, axis=-1, keepdims=True))
    results = [pltpu.make_async_copy(latent_grad, latent_out, lsem.at[7])]
    results[0].start()

    mark("gain1")
    others(lambda k, t: first_round(k, t).wait_recv())
    g_in[0] = g_part[...]
    total = g_in[lax.rem(s + n, n)]
    for t in range(1, n):
        total = total + g_in[lax.rem(s - t + n, n)]
    g_part2[...] = total
    second_round = [rcopy(g_part2, g_in2.at[k], bsend.at[k], brecv.at[k], (s, lax.rem(d + k, m))) for k in range(1, m)]
    for copy in second_round:
        copy.start()

    mark("dr_sum")
    others(lambda k, t: dr_copy(k, t).wait_recv())
    total = dr_in[0]
    for t in range(1, n):
        total = total + dr_in[t]
    summed_dr = jnp.concatenate([total[:, j * ROPE : (j + 1) * ROPE] for j in range(4)], axis=0)
    half = ROPE // 2
    co, si = tc_s[block(s), :half], ts_s[block(s), half:ROPE]
    a, b = summed_dr[:, :half], summed_dr[:, half:]
    rope_grad[...] = jnp.concatenate([a * co + b * si, b * co - a * si], axis=1).T
    results.append(pltpu.make_async_copy(rope_grad, rope_out, lsem.at[8]))
    results[1].start()

    mark("dq_wait")
    for p in range(pairs):
        if has_dq(p):
            others(lambda k, t: returned(p, 2, k, t).wait_recv())
    mark("wgo_wait")
    for p in range(m):
        @pl.when(p != d)
        def _():
            for place in range(ratio):
                rcopy(summed, place_of(place, p), osend.at[0], orecv.at[place, p], (s, p)).wait_recv()
    for copy in second_round:
        copy.wait_recv()
    g_in2[0] = g_part2[...]
    total = g_in2[lax.rem(d + m, m)]
    for t in range(1, m):
        total = total + g_in2[lax.rem(d - t + m, m)]
    for i in range(channels // LANES):
        gain_grad[:, i * LANES : (i + 1) * LANES] = total[i : i + 1, :]
    results.append(pltpu.make_async_copy(gain_grad, gain_out, lsem.at[9]))
    results[2].start()

    mark("drain")
    for g in gs:
        g.finish()
    for w in ws:
        w.finish()
    wg.finish()
    def sent(k, t):
        for chunk in range(len(pn.chunks)):
            for copy in moved(chunk, k, t):
                copy.wait_send()
        for p in range(pairs):
            for i in range(3 if has_dq(p) else 2):
                returned(p, i, k, t).wait_send()
        dr_copy(k, t).wait_send()
        first_round(k, t).wait_send()

    others(sent)
    for t in range(m):
        @pl.when(t != d)
        def _():
            part_copy(t, d).wait_send()
    for copy in second_round:
        copy.wait_send()
    dq_own().wait()
    for copy in results:
        copy.wait()
    for slot in range(n):
        owner, place = slot // ratio, slot % ratio

        @pl.when(owner != d)
        def _():
            rcopy(summed, place_of(slot, d), osend.at[slot], orecv.at[place, d], (s, owner)).wait_send()

        @pl.when(owner == d)
        def _():
            pltpu.make_async_copy(summed, place_of(slot, d), osend.at[slot]).wait()
    mark(None)


def fused(pn, query, grad, latent, rope_key, gain, kw, vw):
    n, m, tokens, channels, length, pairs, tile = pn.n, pn.m, pn.tokens, pn.channels, pn.length, pn.pairs, pn.tile
    cos_t, sin_t = tables(length)
    A = pl.BlockSpec(memory_space=pl.ANY)
    V = pl.BlockSpec(memory_space=pltpu.VMEM)
    S = pltpu.SemaphoreType.DMA
    M = pltpu.VMEM
    piece = (pn.rows, channels)
    held = (pn.depth, (pn.blocks + 1) // 2, tile, (pn.blocks + 1) * tile) if pn.hold else (1, pn.blocks, tile, tile)
    acc = (8, LANES) if pn.hold else (length, LANES)
    outs = (
        jax.ShapeDtypeStruct((tokens, n * pn.qw) if pn.aligned else (n, tokens, pn.qw), bf16),
        jax.ShapeDtypeStruct((2, pn.ratio * pn.own, channels), bf16),
        jax.ShapeDtypeStruct((tokens, channels), f32),
        jax.ShapeDtypeStruct((ROPE, tokens), f32),
        jax.ShapeDtypeStruct((1, channels), f32),
    )
    scratch = [
        M((length, pn.wide), bf16), M((length, channels + LANES), bf16), M((m, *kw.shape), bf16), M((m, *vw.shape), bf16),
        M((2, length, LANES), bf16), M((length, LANES), bf16), M((2, length, LANES), bf16), M((2, LANES, length), bf16), M((2, length, LANES), bf16),
        M((pn.depth, length, tile), f32), M((pn.depth, length, tile), f32), M(held, bf16), M(held, bf16),
        M((pairs, 2 * WIDTH, length), bf16), M((length, LANES), f32), M((length, LANES), f32),
        M((tokens, channels), f32), M((ROPE, tokens), f32), M((1, channels), f32), M(acc, f32), M(acc, f32),
        M((length, pn.qw), bf16), M((pairs, length, LANES), bf16), M((pairs, length, LANES), bf16),
        M((length, LANES), f32), M((n, tokens // 4, LANES), f32), M((n, tokens // 4, LANES), f32),
        M((tokens, n * pn.own), bf16), M((tokens, n * pn.own), bf16),
        M((m, *piece), bf16), M((m, *piece), bf16), M(piece, bf16), M((n, *piece), bf16), M((tokens, channels), f32),
        M((channels // LANES, LANES), f32), M((n, channels // LANES, LANES), f32), M((channels // LANES, LANES), f32), M((m, channels // LANES, LANES), f32),
        S((10,)), S((PARTS, n, 4)), S((PARTS, n)), S((2 * pn.ratio, m, 4)), S((2 * pn.ratio, m)), S((4, n)), S((4, n)), S((3 * pairs, n)), S((3 * pairs, n)),
        S((m,)), S((m,)), S((n, 4)), S((n,)), S((n,)), S((pn.ratio, m)), S((2, n)), S((2, n)), S((m,)), S((m,)),
    ]
    return pl.pallas_call(
        functools.partial(fused_kernel, pn), out_shape=outs,
        in_specs=[A, A, V, V, V, A, A, V, V, V, V], out_specs=(A,) * 5, scratch_shapes=scratch,
        compiler_params=pltpu.CompilerParams(collective_id=11, has_side_effects=True, vmem_limit_bytes=64 * 1024 * 1024 - 64 * 1024),
    )(query, grad, latent, rope_key, gain, kw, vw, jnp.asarray(head_mover(pairs), bf16), jnp.asarray(rope_mover(), bf16), jnp.asarray(cos_t), jnp.asarray(sin_t))


def local(query, latent, rope_key, gain, key_up, value_up, out_grad):
    sp = lax.axis_size("sp")
    dp = lax.axis_size("dp")
    tokens, channels = latent.shape[1:]
    pn = Plan(sp, dp, tokens, channels)
    query, out_grad = pn.pack(query[0], out_grad[0])
    dq, wg, latent_grad, rope_grad, gain_grad = fused(pn, query, out_grad, latent[0], rope_key[0].T, gain[None], key_up, value_up)
    query_grad = dq if pn.aligned else dq.transpose(1, 0, 2).reshape(tokens, -1)
    return (query_grad[None], latent_grad[None], rope_grad.T[None], wg[0].astype(f32), wg[1].astype(f32), gain_grad[0])


def solution(mesh):
    tok = P("dp", "sp", None)
    rows = P("dp", None)
    return jax.shard_map(local, mesh=mesh, in_specs=(tok, tok, tok, P(), rows, rows, tok), out_specs=(tok, tok, tok, rows, rows, P()), check_vma=False)
```

```python
import functools, math
import numpy as np
import jax, jax.numpy as jnp
from jax import lax
from jax.experimental import pallas as pl
from jax.experimental.pallas import tpu as pltpu
from jax.sharding import PartitionSpec as P
ATTENTION_HEADS = 32
PLAIN = 64
ROPE = 32
VALUE = 64
SPAN = 64
WIDTH = PLAIN + ROPE
LANES = 128
NT = (((1,), (1,)), ((), ()))
NN = (((1,), (0,)), ((), ()))
f32=jnp.float32; bf16=jnp.bfloat16
CH=64
MESH = pl.DeviceIdType.MESH
eps = 1e-06


def inner(n):
    return 2 ** ((n.bit_length() - 1) // 2)

def rcopy(src, dst, send, recv, dev):
    return pltpu.make_async_remote_copy(src_ref=src, dst_ref=dst, send_sem=send, recv_sem=recv, device_id=dev, device_id_type=MESH)

class Gather:
    def __init__(self, own, at, na, nb, a, b, dev, send, recv):
        self.own, self.at, self.na, self.nb, self.a, self.b, self.dev, self.send, self.recv = own, at, na, nb, a, b, dev, send, recv
        self.me = a * nb + b
    def copy(self, src, slot, way):
        a, b = self.a, self.b
        to = [(a + 1, b), (a - 1, b), (a, b + 1), (a, b - 1)][way]
        return rcopy(src, self.at(slot), self.send.at[slot, way], self.recv.at[slot], self.dev(*to))
    def can(self, way):
        return [self.a < self.na - 1, self.a > 0, self.b < self.nb - 1, self.b > 0][way]
    def go(self, src, slot, ways):
        for w in ways:
            @pl.when(self.can(w))
            def _(): self.copy(src, slot, w).start()
    def wait(self, slot):
        self.copy(self.own, slot, 0).wait_recv()
    def begin(self):
        self.go(self.own, self.me, (0, 1, 2, 3))
    def line(self, k, got=None):
        for sign, way in ((-1, 0), (1, 1)):
            far = self.a + sign * k
            ok = far >= 0 if sign < 0 else far < self.na
            @pl.when(ok)
            def _():
                slot = far * self.nb + self.b
                self.wait(slot)
                self.go(self.at(slot), slot, (way, 2, 3))
                if got is not None: got(slot)
    def across(self, j, got=None):
        for sign, way in ((-1, 2), (1, 3)):
            far = self.b + sign * j
            ok = far >= 0 if sign < 0 else far < self.nb
            @pl.when(ok)
            def _():
                for aa in range(self.na):
                    slot = aa * self.nb + far
                    self.wait(slot)
                    self.go(self.at(slot), slot, (way,))
                    if got is not None: got(slot)
    def finish(self):
        for w in range(4):
            @pl.when(self.can(w))
            def _(): self.copy(self.own, self.me, w).wait_send()
        for k in range(1, self.na):
            for sign, way in ((-1, 0), (1, 1)):
                far = self.a + sign * k
                ok = far >= 0 if sign < 0 else far < self.na
                @pl.when(ok)
                def _():
                    slot = far * self.nb + self.b
                    for w in (way, 2, 3):
                        @pl.when(self.can(w))
                        def _(): self.copy(self.own, slot, w).wait_send()
        for j in range(1, self.nb - 1):
            for sign, way in ((-1, 2), (1, 3)):
                far = self.b + sign * j
                ok = far >= 0 if sign < 0 else far < self.nb
                @pl.when(ok)
                def _():
                    for aa in range(self.na):
                        slot = aa * self.nb + far
                        @pl.when(self.can(way))
                        def _(): self.copy(self.own, slot, way).wait_send()


def mm(a, b, dims=NN):
    return lax.dot_general(a, b, dims, preferred_element_type=jnp.float32)

def weave(gens):
    gens = list(gens)
    while gens:
        for g in list(gens):
            try: next(g)
            except StopIteration: gens.remove(g)

def pair_backward(tile, heads, cos_t, sin_t, s_s, dp_s, p_s, ds_s, dk_s=None, dv_s=None):
    length = heads[0][3].shape[0]
    blocks = length // tile
    scale = WIDTH ** (-0.5)
    steep = scale * math.log2(math.e)
    depth, held = s_s.shape[0], p_s.shape[0]
    half = ROPE // 2
    query_seg = lax.broadcasted_iota(jnp.int32, (8, tile), 1) // SPAN
    def at(b): return slice(b * tile, (b + 1) * tile)
    half_rows = (blocks + 1) // 2
    def spot(kb, qi, count=1):
        if dk_s is not None:
            return kb, slice(0, tile)
        if kb < half_rows:
            row, col = kb, qi - kb
        else:
            row, col = blocks - 1 - kb, kb + 1 + qi - kb
        return row, slice(col * tile, (col + count) * tile)
    def fold(x, op):
        return op(x.reshape(x.shape[0] // 8, 8, tile), axis=0)
    peaks = {}
    items = [(h, qi) for h in range(len(heads)) for qi in range(blocks)]
    def first(n):
        h, qi = items[n]; odd, q_s, go_s, k_s, kt_s, v_s, _, _ = heads[h]
        q = q_s[at(qi), :]; go = go_s[at(qi), :]
        par = n % depth
        peak = None
        for kb in range(qi + 1):
            s = mm(k_s[at(kb), :], q, NT)
            if kb == qi:
                parts = []
                for j in range(tile // SPAN):
                    ok = jnp.broadcast_to((query_seg >= j)[None], (SPAN // 8, 8, tile)).reshape(SPAN, tile)
                    parts.append(jnp.where(ok, s[j * SPAN:(j + 1) * SPAN], -1e30))
                s = jnp.concatenate(parts, axis=0)
            s_s[par, at(kb), :] = s
            m = fold(s, jnp.max)
            peak = m if peak is None else jnp.maximum(peak, m)
            peaks[n] = peak
            yield
            dp_s[par, at(kb), :] = mm(v_s[at(kb), :], go, NT)
            yield
    def second(n):
        h, qi = items[n]; odd, q_s, go_s, k_s, kt_s, v_s, put_dq, _ = heads[h]
        par = n % depth
        top = jnp.max(peaks[n], axis=0, keepdims=True) * steep
        total = jnp.zeros((8, tile), f32); mixed = jnp.zeros((8, tile), f32)
        for c in range((qi + 1) * tile // CH):
            r = slice(c * CH, (c + 1) * CH)
            p = jnp.exp2(s_s[par, r, :] * steep - top)
            s_s[par, r, :] = p
            total = total + fold(p, jnp.sum)
            mixed = mixed + fold(p * dp_s[par, r, :], jnp.sum)
            if c % (tile // CH) == tile // CH - 1: yield
        inverse = 1.0 / jnp.sum(total, axis=0, keepdims=True)
        delta = jnp.sum(mixed, axis=0, keepdims=True) * inverse
        for c in range((qi + 1) * tile // CH):
            r = slice(c * CH, (c + 1) * CH)
            probs = s_s[par, r, :] * inverse
            kb, inside = divmod(c * CH, tile)
            row, cols = spot(kb, qi)
            p_s[h % held, row, inside : inside + CH, cols] = probs.astype(bf16)
            ds_s[h % held, row, inside : inside + CH, cols] = (probs * (dp_s[par, r, :] - delta)).astype(bf16)
            if c % (tile // CH) == tile // CH - 1: yield
        dq = None
        for kb in range(qi + 1):
            row, cols = spot(kb, qi)
            term = mm(kt_s[:, at(kb)], ds_s[h % held, row, :, cols])
            dq = term if dq is None else dq + term
        dq = dq * scale
        a = 0 if odd else PLAIN
        c_, s_ = cos_t[:, at(qi)], sin_t[:, at(qi)]
        x, y = dq[a : a + half], dq[a + half : a + ROPE]
        b = PLAIN if odd else 0
        if dk_s is not None:
            for kb in range(qi + 1):
                row, cols = spot(kb, qi)
                for acc, left, right in ((dv_s, p_s, go_s), (dk_s, ds_s, q_s)):
                    term = mm(left[h % held, row, :, cols], right[at(qi), :])
                    if kb == qi:
                        acc[at(kb), :] = term
                    else:
                        acc[at(kb), :] += term
        put_dq(at(qi), dq[b : b + PLAIN].astype(bf16), jnp.concatenate([x * c_ + y * s_, y * c_ - x * s_], axis=0).astype(bf16))
        yield
    def last(h):
        odd, q_s, go_s, k_s, kt_s, v_s, _, put_kv = heads[h]
        for kb in range(blocks):
            if dk_s is not None:
                put_kv(at(kb), dk_s[at(kb), :] * scale, dv_s[at(kb), :])
                continue
            row, cols = spot(kb, kb, blocks - kb)
            dv = mm(p_s[h % held, row, :, cols], go_s[kb * tile :, :])
            dk = mm(ds_s[h % held, row, :, cols], q_s[kb * tile :, :])
            put_kv(at(kb), dk * scale, dv)
            yield
    weave([first(0)])
    for n, (h, qi) in enumerate(items):
        gens = [second(n)]
        if n + 1 < len(items): gens.append(first(n + 1))
        weave(gens)
        if qi == blocks - 1: weave([last(h)])

def tables(length):
    inverse = 1.0 / 10000.0 ** (np.arange(0, ROPE, 2, dtype=np.float32) / np.float32(ROPE))
    turned = np.arange(length, dtype=np.float32)[None, :] * inverse.astype(np.float32)[:, None]
    return np.cos(turned.astype(np.float64)).astype(np.float32), np.sin(turned.astype(np.float64)).astype(np.float32)

PARTS = 2


def head_mover(pairs):
    m = np.zeros((min(pairs, 2), 2 * LANES, 4 * LANES), np.float32)
    for p in range(m.shape[0]):
        for h in range(2):
            base = p * 64 + h * WIDTH
            plain, turned = PLAIN * h, PLAIN - PLAIN * h
            for i in range(PLAIN):
                m[p, base + i, 2 * LANES * h + plain + i] = 1
            for i in range(ROPE):
                m[p, base + PLAIN + i, 2 * LANES * h + turned + i] = 1
                m[p, base + PLAIN + (i + ROPE // 2) % ROPE, 2 * LANES * h + LANES + turned + i] = 1
    return m


def rope_unfold():
    m = np.zeros((4, LANES, LANES), np.float32)
    for j in range(4):
        for i in range(ROPE):
            m[j, j * ROPE + i, i] = m[j, j * ROPE + i, PLAIN + i] = 1
    return m


def rope_mover():
    m = np.zeros((ROPE, 2 * LANES), np.float32)
    for i in range(ROPE):
        for at in (0, PLAIN):
            m[i, at + i] = 1
            m[(i + ROPE // 2) % ROPE, LANES + at + i] = 1
    return m


class Plan:
    def __init__(self, n, m, tokens, channels):
        self.n, self.m, self.tokens, self.channels = n, m, tokens, channels
        self.length = n * tokens
        self.heads = ATTENTION_HEADS // n
        self.pairs = self.heads // 2
        self.ratio = n // m
        self.qw = self.heads * WIDTH
        self.own = self.heads * PLAIN
        self.tile = 256
        self.blocks = self.length // self.tile
        self.depth = 2 if self.length <= 2048 else 1
        self.hold = self.length <= 2048
        self.aligned = self.qw % LANES == 0
        qt = -(-self.qw // LANES)
        if self.pairs == 2 and self.qw == 3 * LANES:
            self.chunks = ((0, 3 * LANES), (3 * LANES, 5 * LANES))
            self.q_tiles = ((0, 1), (1, 3))
            self.go_tile = (2, 4)
            self.dq_cols = ((0, LANES), (LANES, 3 * LANES))
        else:
            self.chunks = ((0, (qt + self.pairs) * LANES),)
            self.q_tiles = tuple((p * 2 * WIDTH // LANES, p * 2 * WIDTH // LANES + 1) for p in range(self.pairs))
            self.go_tile = tuple(qt + p for p in range(self.pairs))
            self.dq_cols = ((0, 0),) * (self.pairs - 1) + ((0, self.qw),)
        self.wide = self.chunks[-1][1]
        self.direct = self.pairs == 2 and self.qw == 3 * LANES
        if self.direct:
            self.moves = (((0, 0, 2 * LANES, 0), (1, 0, LANES, 2 * LANES)), ((0, 2 * LANES, LANES, 3 * LANES), (1, LANES, LANES, 4 * LANES)))
        else:
            self.moves = (((2, 0, self.wide, 0),),)
            self.chunks = ((0, self.wide),)
        self.rows = 2 * self.own // m

    def pack(self, query, grad):
        if self.direct:
            return query, grad
        q = query.reshape(self.tokens, self.n, self.qw)
        g = grad.reshape(self.tokens, self.n, self.own)
        gap = self.wide - self.qw - self.own
        parts = [q] + ([jnp.zeros((*q.shape[:2], gap), bf16)] if gap else []) + [g]
        return jnp.concatenate(parts, axis=-1).transpose(1, 0, 2), grad


def fused_kernel(
    pn,
    query, grad, latent, rope_key, gain, kw, vw, move, rmove, unfold, cos_t, sin_t,
    dq_in, wg_out, latent_out, rope_out, gain_out,
    arrived, nlat_all, rope_all, rope2, k_all, v_all, q_s, go_s, k_s, kt_s, v_s, s_s, dp_s, p_s, ds_s, dqt_s, tc_s, ts_s,
    latent_grad, rope_grad, gain_grad, dk_s, dv_s, dq_send, dk_send, dv_send, dr_s, dr_send, dr_in, dk_in, dv_in, part, pieces, summed, blocks, d_nlat, g_part, g_in, g_part2, g_in2,
    lsem, nsend, nrecv, wsend, wrecv, qsend, qrecv, rsend, rrecv, psend, precv, gsend, grecv, osend, orecv, asend, arecv, bsend, brecv,
):
    n, m, tokens, channels, tile = pn.n, pn.m, pn.tokens, pn.channels, pn.tile
    length, pairs, ratio, own = pn.length, pn.pairs, pn.ratio, pn.own
    s = lax.axis_index("sp")
    d = lax.axis_index("dp")
    ny = inner(n)
    nz = n // ny
    z, y = lax.div(s, ny), lax.rem(s, ny)
    x, c = lax.div(d, 2), lax.rem(d, 2)
    scale = WIDTH ** (-0.5)

    scopes = []

    def mark(name):
        if scopes:
            scopes.pop().__exit__(None, None, None)
        if name:
            scopes.append(jax.named_scope(name))
            scopes[-1].__enter__()

    def block(t):
        return pl.ds(pl.multiple_of(t * tokens, tokens), tokens)

    def at(b):
        return slice(b * tile, (b + 1) * tile)

    def source(move, t):
        which, lo, width, _ = move
        if which == 2:
            return query.at[t]
        ref, each = (query, pn.qw) if which == 0 else (grad, own)
        return ref.at[:, pl.ds(pl.multiple_of(t * each + lo, LANES), width)]

    def landing(move, t):
        return arrived.at[block(t), move[3] : move[3] + move[2]]

    spread = [(i, move) for i, moves in enumerate(pn.moves) for move in moves]

    def local_copies():
        made = [pltpu.make_async_copy(kw, k_all.at[d], lsem.at[0]), pltpu.make_async_copy(vw, v_all.at[d], lsem.at[1])]
        return made + [pltpu.make_async_copy(source(move, s), landing(move, s), lsem.at[3 + j]) for j, (_, move) in enumerate(spread)]

    for copy in local_copies():
        copy.start()
    mark("greet")
    bar = pltpu.get_barrier_semaphore()
    for k in range(1, n):
        pl.semaphore_signal(bar, inc=1, device_id=(lax.rem(s + k, n), d), device_id_type=MESH)
    for k in range(1, m):
        pl.semaphore_signal(bar, inc=1, device_id=(s, lax.rem(d + k, m)), device_id_type=MESH)

    lat = latent[...].astype(f32)
    inv_rms = lax.rsqrt(jnp.mean(lat * lat, axis=-1, keepdims=True) + eps)
    nlat_all[block(s), :] = (lat * inv_rms * gain[...]).astype(bf16)
    for b in range(pn.blocks):
        none = jnp.zeros((ROPE, tile), f32)
        co, si = cos_t[:, at(b)], sin_t[:, at(b)]
        tc_s[at(b), :] = jnp.concatenate([co, co, none, co, co, none], axis=0).T
        ts_s[at(b), :] = jnp.concatenate([-si, si, none, -si, si, none], axis=0).T
    turned = mm(rope_key[...], rmove[...], (((0,), (0,)), ((), ())))
    turned = turned[:, :LANES] * tc_s[block(s), :] + turned[:, LANES:] * ts_s[block(s), :]
    quarter = tokens // 4

    def four(t):
        return pl.ds(pl.multiple_of(t * quarter, quarter), quarter)

    rope_all[four(s), :] = jnp.concatenate([turned[j * quarter : (j + 1) * quarter, :ROPE] for j in range(4)], axis=1).astype(bf16)
    dr_s[...] = jnp.zeros_like(dr_s)
    mark("bar_wait")
    pl.semaphore_wait(bar, n + m - 2)

    def member(a, b):
        return (a * ny + b, d)

    gs = []
    cut = tokens // PARTS
    for j in range(PARTS):
        def rows_of(t, j=j):
            return nlat_all.at[pl.ds(pl.multiple_of(t * tokens + j * cut, cut), cut)]
        gs.append(Gather(rows_of(s), rows_of, nz, ny, z, y, member, nsend.at[j], nrecv.at[j]))
    gs.append(Gather(rope_all.at[four(s)], lambda t: rope_all.at[four(t)], nz, ny, z, y, member, nsend.at[PARTS], nrecv.at[PARTS]))
    ws = []
    for j in range(ratio):
        rows = pl.ds(pl.multiple_of(lax.rem(s + j, ratio) * own, own), own)
        for i, (mine, whole) in enumerate(((kw, k_all), (vw, v_all))):
            ws.append(Gather(mine.at[rows], lambda t, whole=whole, rows=rows: whole.at[t, rows], m // 2, 2, x, c,
                             lambda a, b: (s, a * 2 + b), wsend.at[2 * j + i], wrecv.at[2 * j + i]))

    def others(act):
        lax.fori_loop(1, n, lambda k, _: (act(k, lax.rem(s + k, n)), 0)[1], 0)

    def moved(chunk, k, t):
        return [rcopy(source(move, t), landing(move, s), qsend.at[j, k], qrecv.at[j, k], (t, d)) for j, (i, move) in enumerate(spread) if i == chunk]

    def start_moved(chunk, when=None):
        def act(k, t):
            def go():
                for copy in moved(chunk, k, t):
                    copy.start()
            if when is None:
                go()
            else:
                pl.when(when(lax.div(t, ny)))(go)
        others(act)

    mark("gather")
    for g in gs:
        g.begin()
    for w in ws:
        w.begin()
    for i in range(nz):
        if i:
            for g in gs:
                g.line(i)

        @pl.when(z == i)
        def _():
            start_moved(0, lambda tz: tz > z)

        @pl.when(nz - 1 - z == i)
        def _():
            start_moved(0, lambda tz: tz < z)

    start_moved(0, lambda tz: tz == z)
    for chunk in range(1, len(pn.chunks)):
        start_moved(chunk)
    holder = lax.div(s, ratio)
    mine = pl.ds(pl.multiple_of(lax.rem(s, ratio) * own, own), own)

    def project(t):
        rows = block(t)
        a = nlat_all[rows, :]
        keys = mm(a, k_all[holder, mine, :], NT).astype(bf16)
        vals = mm(a, v_all[holder, mine, :], NT).astype(bf16)
        for p in range(pairs):
            dk_send[p, rows, :] = keys[:, p * LANES : (p + 1) * LANES]
            dv_send[p, rows, :] = vals[:, p * LANES : (p + 1) * LANES]

    mark("w_line")
    for w in ws[:2]:
        for k in range(1, m // 2):
            w.line(k)
    for w in ws[:2]:
        w.across(1)
    for copy in local_copies():
        copy.wait()
    mark("project1")
    lax.fori_loop(0, nz, lambda a, _: (project(a * ny + y), 0)[1], 0)
    mark("across")
    for j in range(1, ny):
        for g in gs:
            g.across(j)
    for w in ws[2:]:
        for k in range(1, m // 2):
            w.line(k)
    mark("project2")

    def rest(t, _):
        @pl.when(lax.rem(t, ny) != y)
        def _():
            project(t)
        return 0

    lax.fori_loop(0, n, rest, 0)
    for j in range(4):
        out = mm(rope_all[...], unfold[j]).astype(bf16)
        for t in range(n):
            rope2[t * tokens + j * quarter : t * tokens + (j + 1) * quarter, :] = out[t * quarter : (t + 1) * quarter]

    lane = lax.broadcasted_iota(jnp.int32, (tile, LANES), 1)
    low = lane < PLAIN

    def returned(p, i, k, t):
        lo, hi = pn.dq_cols[p]
        cols = pl.ds(pl.multiple_of(s * own + p * LANES, LANES), LANES)
        if i == 0:
            src, dst = dk_send.at[p, block(t)], dk_in.at[:, cols]
        elif i == 1:
            src, dst = dv_send.at[p, block(t)], dv_in.at[:, cols]
        else:
            src = dq_send.at[block(t), lo:hi]
            dst = dq_in.at[:, pl.ds(pl.multiple_of(s * pn.qw + lo, LANES), hi - lo)] if pn.aligned else dq_in.at[s]
        return rcopy(src, dst, rsend.at[3 * p + i, k], rrecv.at[3 * p + i, k], (t, d))

    def has_dq(p):
        return pn.dq_cols[p][1] > pn.dq_cols[p][0]

    def own_copies(p):
        cols = pl.ds(pl.multiple_of(s * own + p * LANES, LANES), LANES)
        dk_in[:, cols] = dk_send[p, block(s), :]
        dv_in[:, cols] = dv_send[p, block(s), :]

    def dq_own():
        if pn.aligned:
            return pltpu.make_async_copy(dq_send.at[block(s)], dq_in.at[:, pl.ds(pl.multiple_of(s * pn.qw, LANES), pn.qw)], lsem.at[2])
        return pltpu.make_async_copy(dq_send.at[block(s)], dq_in.at[s], lsem.at[2])

    def pieces_of(p):
        return [t for t in range(m) if t * pn.rows // LANES % pairs == p]

    def part_copy(t, j):
        return rcopy(part.at[t], pieces.at[j], psend.at[t], precv.at[j], (s, t))

    def weight_parts(p):
        for i, src in ((p, dk_send), (pairs + p, dv_send)):
            out = mm(src[p], nlat_all[...], (((0,), (0,)), ((), ()))).astype(bf16)
            for r in range(0, LANES, pn.rows):
                part[(i * LANES + r) // pn.rows] = out[r : r + pn.rows]
        for t in pieces_of(p):
            @pl.when(t != d)
            def _():
                part_copy(t, d).start()

    def pair(p, _):
        for q in range(pairs):
            @pl.when(p == q)
            def _():
                if q < len(pn.chunks):
                    with jax.named_scope(f"chunk_wait{q}"):
                        others(lambda k, t: [copy.wait_recv() for copy in moved(q, k, t)])
                t0, t1 = pn.q_tiles[q]

                def prepare(b, _):
                    rows = pl.ds(pl.multiple_of(b * tile, tile), tile)
                    xs = jnp.concatenate([arrived[rows, t0 * LANES : (t0 + 1) * LANES], arrived[rows, t1 * LANES : (t1 + 1) * LANES]], axis=1)
                    out = mm(xs, move[q % 2])
                    tc, ts = tc_s[rows, :], ts_s[rows, :]
                    q_s[0, rows, :] = (out[:, :LANES] * jnp.where(low, 1.0, tc) + out[:, LANES : 2 * LANES] * ts).astype(bf16)
                    q_s[1, rows, :] = (out[:, 2 * LANES : 3 * LANES] * jnp.where(low, tc, 1.0) + out[:, 3 * LANES :] * ts).astype(bf16)
                    go_s[rows, :] = arrived[rows, pn.go_tile[q] * LANES : (pn.go_tile[q] + 1) * LANES]
                    return 0

                lax.fori_loop(0, pn.blocks, prepare, 0)

        for b in range(pn.blocks):
            kp, vp, rp = dk_send[p, at(b), :], dv_send[p, at(b), :], rope2[at(b), :]
            none = jnp.zeros_like(vp)
            even, odd = jnp.where(low, kp, rp), jnp.where(low, rp, kp)
            k_s[0, at(b), :] = even
            k_s[1, at(b), :] = odd
            kt_s[0, :, at(b)] = even.astype(f32).T.astype(bf16)
            kt_s[1, :, at(b)] = odd.astype(f32).T.astype(bf16)
            v_s[0, at(b), :] = jnp.where(low, vp, none)
            v_s[1, at(b), :] = jnp.where(low, none, vp)

        def put_dq(h):
            def put(cols, plain, back):
                dqt_s[p, h * WIDTH : h * WIDTH + PLAIN, cols] = plain
                dqt_s[p, h * WIDTH + PLAIN : (h + 1) * WIDTH, cols] = back
            return put

        def put_kv(h):
            def put(rows, dk, dv):
                if h == 0:
                    dk_send[p, rows, :] = dk.astype(bf16)
                    dv_send[p, rows, :] = dv.astype(bf16)
                    dr_s[rows, :] += jnp.where(low, 0.0, dk)
                else:
                    dk_send[p, rows, :] = jnp.where(low, dk_send[p, rows, :], dk.astype(bf16))
                    dv_send[p, rows, :] = jnp.where(low, dv_send[p, rows, :], dv.astype(bf16))
                    dr_s[rows, :] += jnp.where(low, dk, 0.0)
            return put

        with jax.named_scope("core"):
          pair_backward(tile, [(h == 1, q_s.at[h], go_s, k_s.at[h], kt_s.at[h], v_s.at[h], put_dq(h), put_kv(h)) for h in range(2)],
                      cos_t, sin_t, s_s, dp_s, p_s, ds_s, *(() if pn.hold else (dk_s, dv_s)))

        for q in range(pairs):
            @pl.when(p == q)
            def _():
                lo, hi = pn.dq_cols[q]
                for b in range(pn.blocks):
                    if hi > lo:
                        rows = [dqt_s[i // (2 * WIDTH), i % (2 * WIDTH) : i % (2 * WIDTH) + 64, at(b)] for i in range(lo, hi, 64)]
                        dq_send[at(b), lo:hi] = jnp.concatenate(rows, axis=0).astype(f32).T.astype(bf16)
                if q < pairs - 1:
                    for i in range(3 if has_dq(q) else 2):
                        others(lambda k, t: returned(q, i, k, t).start())
                own_copies(q)
                weight_parts(q)
        return 0

    mark("pairs")
    lax.fori_loop(0, pairs, pair, 0)

    mark("dr")
    both = dr_s[:, :ROPE] + dr_s[:, PLAIN : PLAIN + ROPE]
    for t in range(n):
        dr_send[t] = jnp.concatenate([both[t * tokens + j * quarter : t * tokens + (j + 1) * quarter] for j in range(4)], axis=1).astype(bf16)
    dr_in[s] = dr_send[s]

    def dr_copy(k, t):
        return rcopy(dr_send.at[t], dr_in.at[s], asend.at[1, k], arecv.at[1, k], (t, d))


    final = pairs - 1
    others(lambda k, t: returned(final, 0, k, t).start())
    mark("part_wait")
    pieces[d] = part[d]
    for j in range(m):
        @pl.when(j != d)
        def _():
            part_copy(0, j).wait_recv()
    total = pieces[0].astype(f32)
    for j in range(1, m):
        total = total + pieces[j].astype(f32)
    summed[...] = total.astype(bf16)

    wg = Gather(summed, lambda t: blocks.at[t], nz, ny, z, y, member, gsend, grecv)

    def place_of(slot, j):
        rows = pl.ds(pl.multiple_of(lax.rem(slot, ratio) * own + lax.rem(j, m // 2) * pn.rows, pn.rows), pn.rows)
        return wg_out.at[lax.div(j, m // 2), rows]

    def pass_on(slot, src):
        owner, place = lax.div(slot, ratio), lax.rem(slot, ratio)

        @pl.when(owner != d)
        def _():
            rcopy(src, place_of(slot, d), osend.at[slot], orecv.at[place, d], (s, owner)).start()

        @pl.when(owner == d)
        def _():
            pltpu.make_async_copy(src, place_of(slot, d), osend.at[slot]).start()

    mark("wg_line")
    wg.begin()
    pass_on(s, summed)
    dq_own().start()
    others(lambda k, t: returned(final, 1, k, t).start())
    results = []

    def first_round(k, t):
        return rcopy(g_part, g_in.at[k], asend.at[0, k], arecv.at[0, k], (t, d))

    def turn_back():
        mark("kv_wait")
        for p in range(pairs):
            for i in range(2):
                others(lambda k, t: returned(p, i, k, t).wait_recv())
        mark("w_rest")
        for w in ws[2:]:
            w.across(1)
        mark("d_nlat")
        for t in range(m):
            cols = slice(t * ratio * own, (t + 1) * ratio * own)
            term = mm(dk_in[:, cols], k_all[t]) + mm(dv_in[:, cols], v_all[t])
            if t == 0:
                d_nlat[...] = term
            else:
                d_nlat[...] += term
        lat = latent[...].astype(f32)
        inv_rms = lax.rsqrt(jnp.mean(lat * lat, axis=-1, keepdims=True) + eps)
        normed = lat * inv_rms
        dn = d_nlat[...]
        sums = jnp.sum(dn * normed, axis=0, keepdims=True)
        g_part[...] = jnp.concatenate([sums[:, i * LANES : (i + 1) * LANES] for i in range(channels // LANES)], axis=0)
        others(lambda k, t: first_round(k, t).start())
        scaled = dn * gain[...]
        latent_grad[...] = inv_rms * (scaled - normed * jnp.mean(scaled * normed, axis=-1, keepdims=True))
        results.append(pltpu.make_async_copy(latent_grad, latent_out, lsem.at[7]))
        results[-1].start()

    def send_dq(when):
        def act(k, t):
            @pl.when(when(lax.div(t, ny)))
            def _():
                returned(final, 2, k, t).start()
        others(act)

    for i in range(nz):
        if i:
            if i == nz - 1:
                turn_back()
                mark("wg_last")
            wg.line(i, lambda slot: pass_on(slot, blocks.at[slot]))
        if i == 1:
            others(lambda k, t: dr_copy(k, t).start())

        @pl.when(z == i)
        def _():
            send_dq(lambda tz: tz > z)

        @pl.when(nz - 1 - z == i)
        def _():
            send_dq(lambda tz: tz < z)

    send_dq(lambda tz: tz == z)
    mark("wg_across")
    for j in range(1, ny):
        wg.across(j, lambda slot: pass_on(slot, blocks.at[slot]))
    mark("gain1")
    others(lambda k, t: first_round(k, t).wait_recv())
    g_in[0] = g_part[...]
    total = g_in[lax.rem(s + n, n)]
    for t in range(1, n):
        total = total + g_in[lax.rem(s - t + n, n)]
    g_part2[...] = total
    second_round = [rcopy(g_part2, g_in2.at[k], bsend.at[k], brecv.at[k], (s, lax.rem(d + k, m))) for k in range(1, m)]
    for copy in second_round:
        copy.start()

    mark("dr_sum")
    others(lambda k, t: dr_copy(k, t).wait_recv())
    total = dr_in[0].astype(f32)
    for t in range(1, n):
        total = total + dr_in[t].astype(f32)
    summed_dr = jnp.concatenate([total[:, j * ROPE : (j + 1) * ROPE] for j in range(4)], axis=0)
    half = ROPE // 2
    co, si = tc_s[block(s), :half], ts_s[block(s), half:ROPE]
    a, b = summed_dr[:, :half], summed_dr[:, half:]
    rope_grad[...] = jnp.concatenate([a * co + b * si, b * co - a * si], axis=1).T
    results.append(pltpu.make_async_copy(rope_grad, rope_out, lsem.at[8]))
    results[-1].start()

    mark("dq_wait")
    for p in range(pairs):
        if has_dq(p):
            others(lambda k, t: returned(p, 2, k, t).wait_recv())
    mark("wgo_wait")
    for p in range(m):
        @pl.when(p != d)
        def _():
            for place in range(ratio):
                rcopy(summed, place_of(place, p), osend.at[0], orecv.at[place, p], (s, p)).wait_recv()
    for copy in second_round:
        copy.wait_recv()
    g_in2[0] = g_part2[...]
    total = g_in2[lax.rem(d + m, m)]
    for t in range(1, m):
        total = total + g_in2[lax.rem(d - t + m, m)]
    for i in range(channels // LANES):
        gain_grad[:, i * LANES : (i + 1) * LANES] = total[i : i + 1, :]
    results.append(pltpu.make_async_copy(gain_grad, gain_out, lsem.at[9]))
    results[-1].start()

    mark("drain")
    for g in gs:
        g.finish()
    for w in ws:
        w.finish()
    wg.finish()
    def sent(k, t):
        for chunk in range(len(pn.chunks)):
            for copy in moved(chunk, k, t):
                copy.wait_send()
        for p in range(pairs):
            for i in range(3 if has_dq(p) else 2):
                returned(p, i, k, t).wait_send()
        dr_copy(k, t).wait_send()
        first_round(k, t).wait_send()

    others(sent)
    for t in range(m):
        @pl.when(t != d)
        def _():
            part_copy(t, d).wait_send()
    for copy in second_round:
        copy.wait_send()
    dq_own().wait()
    for copy in results:
        copy.wait()
    for slot in range(n):
        owner, place = slot // ratio, slot % ratio

        @pl.when(owner != d)
        def _():
            rcopy(summed, place_of(slot, d), osend.at[slot], orecv.at[place, d], (s, owner)).wait_send()

        @pl.when(owner == d)
        def _():
            pltpu.make_async_copy(summed, place_of(slot, d), osend.at[slot]).wait()
    mark(None)


def fused(pn, query, grad, latent, rope_key, gain, kw, vw):
    n, m, tokens, channels, length, pairs, tile = pn.n, pn.m, pn.tokens, pn.channels, pn.length, pn.pairs, pn.tile
    cos_t, sin_t = tables(length)
    A = pl.BlockSpec(memory_space=pl.ANY)
    V = pl.BlockSpec(memory_space=pltpu.VMEM)
    S = pltpu.SemaphoreType.DMA
    M = pltpu.VMEM
    piece = (pn.rows, channels)
    held = (pn.depth, (pn.blocks + 1) // 2, tile, (pn.blocks + 1) * tile) if pn.hold else (1, pn.blocks, tile, tile)
    acc = (8, LANES) if pn.hold else (length, LANES)
    outs = (
        jax.ShapeDtypeStruct((tokens, n * pn.qw) if pn.aligned else (n, tokens, pn.qw), bf16),
        jax.ShapeDtypeStruct((2, pn.ratio * pn.own, channels), bf16),
        jax.ShapeDtypeStruct((tokens, channels), f32),
        jax.ShapeDtypeStruct((ROPE, tokens), f32),
        jax.ShapeDtypeStruct((1, channels), f32),
    )
    scratch = [
        M((length, pn.wide), bf16), M((length, channels), bf16), M((length // 4, LANES), bf16), M((length, LANES), bf16), M((m, *kw.shape), bf16), M((m, *vw.shape), bf16),
        M((2, length, LANES), bf16), M((length, LANES), bf16), M((2, length, LANES), bf16), M((2, LANES, length), bf16), M((2, length, LANES), bf16),
        M((pn.depth, length, tile), f32), M((pn.depth, length, tile), f32), M(held, bf16), M(held, bf16),
        M((pairs, 2 * WIDTH, length), bf16), M((length, LANES), f32), M((length, LANES), f32),
        M((tokens, channels), f32), M((ROPE, tokens), f32), M((1, channels), f32), M(acc, f32), M(acc, f32),
        M((length, pn.qw), bf16), M((pairs, length, LANES), bf16), M((pairs, length, LANES), bf16),
        M((length, LANES), f32), M((n, tokens // 4, LANES), bf16), M((n, tokens // 4, LANES), bf16),
        M((tokens, n * pn.own), bf16), M((tokens, n * pn.own), bf16),
        M((m, *piece), bf16), M((m, *piece), bf16), M(piece, bf16), M((n, *piece), bf16), M((tokens, channels), f32),
        M((channels // LANES, LANES), f32), M((n, channels // LANES, LANES), f32), M((channels // LANES, LANES), f32), M((m, channels // LANES, LANES), f32),
        S((10,)), S((PARTS + 1, n, 4)), S((PARTS + 1, n)), S((2 * pn.ratio, m, 4)), S((2 * pn.ratio, m)), S((4, n)), S((4, n)), S((3 * pairs, n)), S((3 * pairs, n)),
        S((m,)), S((m,)), S((n, 4)), S((n,)), S((n,)), S((pn.ratio, m)), S((2, n)), S((2, n)), S((m,)), S((m,)),
    ]
    return pl.pallas_call(
        functools.partial(fused_kernel, pn), out_shape=outs,
        in_specs=[A, A, V, V, V, A, A, V, V, V, V, V], out_specs=(A,) * 5, scratch_shapes=scratch,
        compiler_params=pltpu.CompilerParams(collective_id=11, has_side_effects=True, vmem_limit_bytes=64 * 1024 * 1024 - 64 * 1024),
    )(query, grad, latent, rope_key, gain, kw, vw, jnp.asarray(head_mover(pairs), bf16), jnp.asarray(rope_mover(), bf16), jnp.asarray(rope_unfold(), bf16), jnp.asarray(cos_t), jnp.asarray(sin_t))


def finish_kernel(aligned, *refs):
    if aligned:
        refs[5][...] = refs[4][...]
        refs = refs[:4] + refs[6:]
    wg, latent, rope, gain, kw_out, vw_out, latent_out, rope_out, gain_out = refs
    kw_out[...] = wg[0].astype(f32)
    vw_out[...] = wg[1].astype(f32)
    latent_out[...] = latent[...]
    rope_out[...] = rope[...]
    gain_out[...] = gain[...]


def finish(dq, wg, latent, rope, gain, aligned):
    steps = 4
    weights = (wg.shape[1] // steps, wg.shape[2])

    def rows(a):
        return pl.BlockSpec((a.shape[0] // steps, a.shape[1]), lambda i: (i, 0))

    def whole(a):
        return pl.BlockSpec(a.shape, lambda i: (0, 0))

    first = [dq] if aligned else []
    ins = [wg, latent, rope, gain] + first
    in_specs = [pl.BlockSpec((2, *weights), lambda i: (0, i, 0)), rows(latent), whole(rope), whole(gain)] + [rows(a) for a in first]
    shape = jax.ShapeDtypeStruct(wg.shape[1:], f32)
    outs = [jax.ShapeDtypeStruct(a.shape, a.dtype) for a in first] + [shape, shape] + [jax.ShapeDtypeStruct(a.shape, a.dtype) for a in (latent, rope, gain)]
    out_specs = [rows(a) for a in first] + [rows(shape), rows(shape), rows(latent), whole(rope), whole(gain)]
    done = pl.pallas_call(
        functools.partial(finish_kernel, aligned), grid=(steps,), out_shape=outs, in_specs=in_specs, out_specs=out_specs,
        compiler_params=pltpu.CompilerParams(dimension_semantics=("arbitrary",)),
    )(*ins)
    return done if aligned else [dq] + list(done)


def local(query, latent, rope_key, gain, key_up, value_up, out_grad):
    sp = lax.axis_size("sp")
    dp = lax.axis_size("dp")
    tokens, channels = latent.shape[1:]
    pn = Plan(sp, dp, tokens, channels)
    query, out_grad = pn.pack(query[0], out_grad[0])
    dq, wg, latent_grad, rope_grad, gain_grad = fused(pn, query, out_grad, latent[0], rope_key[0].T, gain[None], key_up, value_up)
    dq, kw, vw, latent_grad, rope_grad, gain_grad = finish(dq, wg, latent_grad, rope_grad, gain_grad, pn.aligned)
    query_grad = dq if pn.aligned else dq.transpose(1, 0, 2).reshape(tokens, -1)
    return (query_grad[None], latent_grad[None], rope_grad.T[None], kw, vw, gain_grad[0])


def solution(mesh):
    tok = P("dp", "sp", None)
    rows = P("dp", None)
    return jax.shard_map(local, mesh=mesh, in_specs=(tok, tok, tok, P(), rows, rows, tok), out_specs=(tok, tok, tok, rows, rows, P()), check_vma=False)
```
